32 devices in a mesh: rep: 2 (over x), fs: 4 (over z), tp: 4 (over y, core).
Axes of the slice: x: 2, y: 2, z: 4, core: 2. Of those that a mesh axis runs over, the one named last changes fastest.
Arguments:
- tokens: bfloat16 [8192, 2048], P(('rep', 'fs'), 'tp'), may hold values from -6 to 6
- mix_gain: float32 [2048], replicated, may hold values from 0.1 to 1.9
- query_weight: bfloat16 [2048, 512], P('fs', 'tp'), may hold values from -0.125 to 0.125
- key_weight: bfloat16 [2048, 512], P('fs', 'tp'), may hold values from -0.125 to 0.125
- value_weight: bfloat16 [2048, 1024], P('fs', 'tp'), may hold values from -0.125 to 0.125
- gate_weight: bfloat16 [2048, 1024], P('fs', 'tp'), may hold values from -0.125 to 0.125
- out_weight: bfloat16 [1024, 2048], P('tp', 'fs'), may hold values from -0.1875 to 0.1875
- head_gain: float32 [8, 128], P('tp'), may hold values from 0.1 to 1.9
- ffn_gain: float32 [2048], replicated, may hold values from 0.1 to 1.9
- ffn_gate: bfloat16 [2048, 5632], P('fs', 'tp'), may hold values from -0.125 to 0.125
- ffn_up: bfloat16 [2048, 5632], P('fs', 'tp'), may hold values from -0.125 to 0.125
- ffn_down: bfloat16 [5632, 2048], P('tp', 'fs'), may hold values from -0.078125 to 0.078125
Outputs:
- layer_out: bfloat16 [8192, 2048], P(('rep', 'fs'), 'tp')
The draws below stay inside these ranges and needn't reach their ends.
All inputs are finite; a program needn't handle non-finite values.
Results may differ from the reference program's by a relative error of at most 0.03.
Values may be sent and summed in bfloat16 or wider, within the bound.
A program may use at most 128 MiB of HBM per device.

```python
import jax
import jax.numpy as jnp
from jax import lax

D = 2048
HEADS = 8
DK = 64
DV = 128
FF = 5632
SEQ = 256
TOKENS = 8192
N_TP = 4


def levels(rng, extent, shards, least, largest):
    gain = 1.0
    for dim, parts in shards:
        steps = jax.random.uniform(jax.random.fold_in(jax.random.fold_in(rng, 6), dim), (parts,), jnp.float32, least / len(shards), largest / len(shards))
        gain = gain * jnp.repeat(jnp.exp(steps), extent[dim] // parts).reshape((-1,) + (1,) * (len(extent) - 1 - dim))
    return gain


def normal_values(key, extent, scale, most, shards=(), held_as=jnp.bfloat16):
    level = levels(key, extent, shards, -0.22, 0.18) if shards else 1.0
    values = jax.random.normal(key, extent, jnp.float32) * scale * level
    return jnp.minimum(jnp.maximum(values, -most), most).astype(held_as)


def setup_inputs(seed: int = 0) -> dict:
    seeds = jax.random.split(jax.random.key(seed), 13)
    return {
        "tokens": normal_values(seeds[0], (TOKENS, D), 1.0, 6.0, ((0, 8), (1, 4))),
        "mix_gain": jnp.clip(1.0 + 0.18 * jax.random.normal(seeds[1], (D,), jnp.float32), 0.1, 1.9),
        "query_weight": normal_values(seeds[2], (D, HEADS * DK), D ** -0.5, 0.125, ((0, 4), (1, 4))),
        "key_weight": normal_values(seeds[3], (D, HEADS * DK), D ** -0.5, 0.125, ((0, 4), (1, 4))),
        "value_weight": normal_values(seeds[4], (D, HEADS * DV), D ** -0.5, 0.125, ((0, 4), (1, 4))),
        "gate_weight": normal_values(seeds[5], (D, HEADS * DV), D ** -0.5, 0.125, ((0, 4), (1, 4))),
        "out_weight": normal_values(seeds[6], (HEADS * DV, D), (HEADS * DV) ** -0.5, 0.1875, ((0, 4), (1, 4))),
        "head_gain": jnp.clip(1.0 + 0.18 * jax.random.normal(seeds[7], (HEADS, DV), jnp.float32), 0.1, 1.9),
        "ffn_gain": jnp.clip(1.0 + 0.18 * jax.random.normal(seeds[8], (D,), jnp.float32), 0.1, 1.9),
        "ffn_gate": normal_values(seeds[9], (D, FF), D ** -0.5, 0.125, ((0, 4), (1, 4))),
        "ffn_up": normal_values(seeds[10], (D, FF), D ** -0.5, 0.125, ((0, 4), (1, 4))),
        "ffn_down": normal_values(seeds[11], (FF, D), FF ** -0.5, 0.078125, ((0, 4), (1, 4))),
    }


epsilon = 1e-06
rope_base = 10000.0

def norm_rows(values, gain_row):
    floats = values.astype(jnp.float32)
    scaled = floats * lax.rsqrt(lax.optimization_barrier(jnp.mean(floats * floats, axis=-1, keepdims=True)) + epsilon)
    return (scaled * gain_row).astype(jnp.bfloat16)

def rotate(values, positions):
    half_dim = values.shape[-1] // 2
    frequency = rope_base ** (-jnp.linspace(0.0, 1.0, half_dim, dtype=jnp.float32))
    angles = positions.astype(jnp.float32)[:, None] * frequency[None, :]
    cosine = jnp.cos(angles)[:, None, :]
    sine_part = jnp.sin(angles)[:, None, :]
    paired = values.reshape(values.shape[:-1] + (half_dim, 2))
    leading = paired[..., 0]
    trailing = paired[..., 1]
    turned = jnp.stack([leading * cosine - trailing * sine_part, leading * sine_part + trailing * cosine], axis=-1)
    return turned.reshape(values.shape)

def log_decay(head_index, total_heads):
    return jnp.log1p(-jnp.exp2(-5.0 - 4.0 * head_index.astype(jnp.float32) / (total_heads - 1)))

def split_sum(left, right):
    columns = left.shape[1] // N_TP
    summed = jnp.zeros((left.shape[0], right.shape[1]), jnp.float32)
    for segment in range(N_TP):
        partial_value = jnp.dot(left[:, segment * columns:(segment + 1) * columns], right[segment * columns:(segment + 1) * columns], preferred_element_type=jnp.float32).astype(jnp.bfloat16)
        summed = summed + lax.optimization_barrier(partial_value).astype(jnp.float32)
    return summed

def reference(tokens, mix_gain, query_weight, key_weight, value_weight, gate_weight, out_weight, head_gain, ffn_gain, ffn_gate, ffn_up, ffn_down):
    highest = lax.Precision.HIGHEST
    row_count = tokens.shape[0]
    normed = norm_rows(tokens, mix_gain)

    def project(weight):
        return jnp.dot(normed, weight, preferred_element_type=jnp.float32).astype(jnp.bfloat16)
    positions = jnp.arange(row_count, dtype=jnp.int32) % SEQ
    queries = rotate(project(query_weight).astype(jnp.float32).reshape(row_count, HEADS, DK), positions)
    key_rows = rotate(project(key_weight).astype(jnp.float32).reshape(row_count, HEADS, DK), positions) * DK ** (-0.5)
    value_rows = project(value_weight).astype(jnp.float32).reshape(row_count, HEADS, DV)
    gate_rows = project(gate_weight).astype(jnp.float32)
    decay_rates = log_decay(jnp.arange(HEADS, dtype=jnp.int32), HEADS)
    offsets = jnp.arange(SEQ, dtype=jnp.int32)
    distance = (offsets[:, None] - offsets[None, :]).astype(jnp.float32)
    decay_mask = jnp.where(distance[None] >= 0.0, jnp.exp(jnp.maximum(distance, 0.0)[None] * decay_rates[:, None, None]), 0.0)
    seq_count = row_count // SEQ

    def one_sequence(inputs):
        query_seq, key_seq, value_seq = inputs
        scores = jnp.einsum('ihd,jhd->hij', query_seq, key_seq, precision=highest) * decay_mask
        return jnp.einsum('hij,jhv->ihv', scores, value_seq, precision=highest)
    retained = lax.map(one_sequence, (queries.reshape(seq_count, SEQ, HEADS, DK), key_rows.reshape(seq_count, SEQ, HEADS, DK), value_rows.reshape(seq_count, SEQ, HEADS, DV)))
    retained = retained.reshape(row_count, HEADS, DV)
    center = lax.optimization_barrier(jnp.mean(retained, axis=-1, keepdims=True))
    spread = lax.optimization_barrier(jnp.mean(jnp.square(retained - center), axis=-1, keepdims=True))
    grouped = (retained - center) * lax.rsqrt(spread + epsilon) * head_gain[None]
    mixed = (grouped.reshape(row_count, HEADS * DV) * jax.nn.silu(gate_rows)).astype(jnp.bfloat16)
    residual = (tokens.astype(jnp.float32) + split_sum(mixed, out_weight)).astype(jnp.bfloat16)
    normed_ffn = norm_rows(residual, ffn_gain)
    gate_hidden = jnp.dot(normed_ffn, ffn_gate, preferred_element_type=jnp.float32)
    up_hidden = jnp.dot(normed_ffn, ffn_up, preferred_element_type=jnp.float32)
    hidden = (jax.nn.silu(gate_hidden) * up_hidden).astype(jnp.bfloat16)
    return (residual.astype(jnp.float32) + split_sum(hidden, ffn_down)).astype(jnp.bfloat16)
```

```python
import jax
import jax.numpy as jnp
import numpy as np
from jax import lax
from jax.experimental import pallas as pl
from jax.experimental.pallas import tpu as pltpu
from jax.sharding import PartitionSpec as P

HEADS = 8
DK = 64
DV = 128
BLOCK = 64
SEQ = 256


epsilon = 1e-06
rope_base = 10000.0


def norm_rows(values, gain_row):
    floats = values.astype(jnp.float32)
    scaled = floats * lax.rsqrt(jnp.mean(floats * floats, axis=-1, keepdims=True) + epsilon)
    return (scaled * gain_row).astype(jnp.bfloat16)


def rotate(values, positions):
    half_dim = values.shape[-1] // 2
    frequency = rope_base ** (-jnp.linspace(0.0, 1.0, half_dim, dtype=jnp.float32))
    angles = positions.astype(jnp.float32)[:, None] * frequency[None, :]
    cosine = jnp.cos(angles)[:, None, :]
    sine_part = jnp.sin(angles)[:, None, :]
    paired = values.reshape(values.shape[:-1] + (half_dim, 2))
    leading = paired[..., 0]
    trailing = paired[..., 1]
    turned = jnp.stack(
        [leading * cosine - trailing * sine_part, leading * sine_part + trailing * cosine], axis=-1
    )
    return turned.reshape(values.shape)


def log_decay(head_index, total_heads):
    return jnp.log1p(-jnp.exp2(-5.0 - 4.0 * head_index.astype(jnp.float32) / (total_heads - 1)))


def retention(queries, key_rows, value_rows, decay_rates):
    highest = lax.Precision.HIGHEST
    row_count, head_count = (queries.shape[0], queries.shape[1])
    seq_count = row_count // SEQ
    block_count = SEQ // BLOCK

    def to_blocks(values):
        shaped = values.reshape((seq_count, block_count, BLOCK) + values.shape[1:])
        return jnp.moveaxis(shaped, 1, 0)

    inside = jnp.arange(BLOCK, dtype=jnp.int32)
    gap = (inside[:, None] - inside[None, :]).astype(jnp.float32)
    within_mask = jnp.where(
        gap[None] >= 0.0, jnp.exp(jnp.maximum(gap, 0.0)[None] * decay_rates[:, None, None]), 0.0
    )
    query_scale = jnp.exp((inside + 1).astype(jnp.float32)[:, None] * decay_rates[None, :])
    key_scale = jnp.exp((BLOCK - 1 - inside).astype(jnp.float32)[:, None] * decay_rates[None, :])
    block_decay = jnp.exp(BLOCK * decay_rates)

    def advance(state, inputs):
        query_blk, key_blk, value_blk = inputs
        scores = (
            jnp.einsum("sihd,sjhd->shij", query_blk, key_blk, precision=highest) * within_mask[None]
        )
        local_part = jnp.einsum("shij,sjhv->sihv", scores, value_blk, precision=highest)
        carried = jnp.einsum(
            "sihd,shdv->sihv", query_blk * query_scale[None, :, :, None], state, precision=highest
        )
        update = jnp.einsum(
            "sjhd,sjhv->shdv", key_blk * key_scale[None, :, :, None], value_blk, precision=highest
        )
        return (block_decay[None, :, None, None] * state + update, local_part + carried)

    state_zero = jnp.zeros((seq_count, head_count, DK, DV), jnp.float32)
    _, outputs = lax.scan(
        advance, state_zero, (to_blocks(queries), to_blocks(key_rows), to_blocks(value_rows))
    )
    return jnp.moveaxis(outputs, 0, 1).reshape(row_count, head_count, DV)


def per_device_plain(
    tokens,
    mix_gain,
    query_weight,
    key_weight,
    value_weight,
    gate_weight,
    out_weight,
    head_gain,
    ffn_gain,
    ffn_gate,
    ffn_up,
    ffn_down,
):
    whole_rows = lax.all_gather(tokens, "tp", axis=1, tiled=True)
    row_count = whole_rows.shape[0]
    normed = norm_rows(whole_rows, mix_gain)
    pieces = (
        lax.all_gather(query_weight, "fs", axis=0, tiled=True),
        lax.all_gather(key_weight, "fs", axis=0, tiled=True),
        lax.all_gather(value_weight, "fs", axis=0, tiled=True),
        lax.all_gather(gate_weight, "fs", axis=0, tiled=True),
    )
    query_acc, key_acc, value_acc, gate_acc = tuple(
        (
            jnp.dot(normed, weight_piece, preferred_element_type=jnp.float32)
            for weight_piece in pieces
        )
    )
    heads_here = query_weight.shape[1] // DK
    positions = jnp.arange(row_count, dtype=jnp.int32) % SEQ
    queries = rotate(
        query_acc.astype(jnp.bfloat16).astype(jnp.float32).reshape(row_count, heads_here, DK),
        positions,
    )
    key_rows = rotate(
        key_acc.astype(jnp.bfloat16).astype(jnp.float32).reshape(row_count, heads_here, DK),
        positions,
    ) * DK ** (-0.5)
    value_rows = (
        value_acc.astype(jnp.bfloat16).astype(jnp.float32).reshape(row_count, heads_here, DV)
    )
    gate_rows = gate_acc.astype(jnp.bfloat16).astype(jnp.float32)
    first_head = lax.axis_index("tp") * heads_here
    decay_rates = log_decay(first_head + jnp.arange(heads_here, dtype=jnp.int32), HEADS)
    retained = retention(queries, key_rows, value_rows, decay_rates)
    center = jnp.mean(retained, axis=-1, keepdims=True)
    spread = jnp.mean(jnp.square(retained - center), axis=-1, keepdims=True)
    grouped = (retained - center) * lax.rsqrt(spread + epsilon) * head_gain[None]
    mixed = (grouped.reshape(row_count, heads_here * DV) * jax.nn.silu(gate_rows)).astype(
        jnp.bfloat16
    )
    mixer_terms = jnp.dot(
        mixed,
        lax.all_gather(out_weight, "fs", axis=1, tiled=True),
        preferred_element_type=jnp.float32,
    )
    mixer_share = lax.psum_scatter(
        mixer_terms.astype(jnp.bfloat16), "tp", scatter_dimension=1, tiled=True
    ).astype(jnp.float32)
    resid_shard = (tokens.astype(jnp.float32) + mixer_share).astype(jnp.bfloat16)
    resid_whole = lax.all_gather(resid_shard, "tp", axis=1, tiled=True)
    normed_ffn = norm_rows(resid_whole, ffn_gain)

    def add_rows(weight_piece):
        return jnp.dot(normed_ffn, weight_piece, preferred_element_type=jnp.float32)

    gate_hidden = add_rows(lax.all_gather(ffn_gate, "fs", axis=0, tiled=True))
    up_hidden = add_rows(lax.all_gather(ffn_up, "fs", axis=0, tiled=True))
    hidden = (jax.nn.silu(gate_hidden) * up_hidden).astype(jnp.bfloat16)
    ffn_terms = jnp.dot(
        hidden,
        lax.all_gather(ffn_down, "fs", axis=1, tiled=True),
        preferred_element_type=jnp.float32,
    )
    ffn_share = lax.psum_scatter(
        ffn_terms.astype(jnp.bfloat16), "tp", scatter_dimension=1, tiled=True
    ).astype(jnp.float32)
    return (resid_shard.astype(jnp.float32) + ffn_share).astype(jnp.bfloat16)


MESH = pl.DeviceIdType.MESH
LANES = 128


def fused_kernel(
    tokens_ref, mix_gain_ref, query_ref, key_ref, value_ref, gate_ref, proj_out_ref, head_gain_ref,
    ffn_gain_ref, ffn_gate_ref, ffn_up_ref, ffn_down_ref, cos_ref, sin_ref, rate_ref,
    out_ref,
    w_mix, w_out, w_ffn, w_down, x_all, res_all, normed, normed_ffn, proj, mixed, hidden, mask,
    corner1, corner1_in, beside1, beside1_in, across1, across1_in, own1,
    corner2, corner2_in, beside2, beside2_in, across2, across2_in, own2,
    local_sem, z_send, z_recv, x_send, x_recv, y_send, y_recv,
):
    f32, bf16 = jnp.float32, jnp.bfloat16
    rep, here, tp = lax.axis_index("rep"), lax.axis_index("fs"), lax.axis_index("tp")
    core, chip = tp % 2, tp // 2
    beside_id, across_id, corner_id = tp + 1 - 2 * core, (tp + 2) % 4, 3 - tp
    rows, width = tokens_ref.shape
    seqs = rows // SEQ
    shard = query_ref.shape[0]
    key_width, value_width = query_ref.shape[1], value_ref.shape[1]
    heads = head_gain_ref.shape[0]
    ffn_blocks = ffn_gate_ref.shape[1] // LANES
    down_chunks = ffn_down_ref.shape[1] // LANES
    pair_width = 2 * LANES

    def own_rows(size, base=None):
        index = here if base is None else base
        return pl.ds(pl.multiple_of(index * size, size), size)

    local = []

    def bring(source, target):
        copy = pltpu.make_async_copy(source, target, local_sem.at[len(local)])
        copy.start()
        local.append(copy)
        return copy

    token_columns = own_rows(width, tp)
    bring_tokens = bring(tokens_ref, x_all.at[:, token_columns])
    bring_mix = []
    start = 0
    for ref in (query_ref, key_ref, value_ref, gate_ref):
        bring_mix.append(bring(ref, w_mix.at[own_rows(shard), pl.ds(start, ref.shape[1])]))
        start += ref.shape[1]
    bring_out = bring(proj_out_ref, w_out.at[:, own_rows(proj_out_ref.shape[1])])
    bring_ffn = []
    for block in range(ffn_blocks):
        pair = []
        for part, ref in enumerate((ffn_gate_ref, ffn_up_ref)):
            pair.append(
                bring(
                    ref.at[:, pl.ds(block * LANES, LANES)],
                    w_ffn.at[own_rows(shard), pl.ds(block * pair_width + part * LANES, LANES)],
                )
            )
        bring_ffn.append(pair)
    bring_down = [
        bring(ffn_down_ref.at[:, pl.ds(c * LANES, LANES)], w_down.at[c, :, own_rows(LANES)])
        for c in range(down_chunks)
    ]

    chunks = []
    mix_chunks = w_mix.shape[1] // pair_width
    half_shard = shard // 2

    def row_chunk(buffer, column):
        def view(s, half):
            first = pl.multiple_of(s * shard + half * half_shard, half_shard)
            return buffer.at[pl.ds(first, half_shard), pl.ds(column, pair_width)]

        return view

    for i in range(mix_chunks):
        needs = {0: bring_mix[:2], 1: bring_mix[2:3], 2: bring_mix[3:]}[i]
        chunks.append((row_chunk(w_mix, i * pair_width), needs))

    def out_view(s, half):
        size, columns = w_out.shape[0] // 2, proj_out_ref.shape[1]
        return w_out.at[own_rows(size, half), own_rows(columns, s)]

    chunks.append((out_view, [bring_out]))
    for block in range(ffn_blocks):
        chunks.append((row_chunk(w_ffn, block * pair_width), bring_ffn[block]))

    def down_view(c):
        def view(s, half):
            size = w_down.shape[1] // 2
            return w_down.at[c, own_rows(size, half), own_rows(LANES, s)]

        return view

    for c in range(down_chunks):
        chunks.append((down_view(c), [bring_down[c]]))
    total = len(chunks)
    first_ffn = mix_chunks + 1
    first_down = first_ffn + ffn_blocks

    barrier = pltpu.get_barrier_semaphore()
    for target in (
        {"fs": (here + 1) % 4}, {"fs": (here + 3) % 4}, {"rep": 1 - rep}, {"tp": beside_id}, {"tp": across_id},
    ):
        pl.semaphore_signal(barrier, inc=1, device_id=target, device_id_type=MESH)
    pl.semaphore_wait(barrier, 5)

    def z_copy(k, d, hop, s, target):
        view = chunks[k][0](s, rep)
        return pltpu.make_async_remote_copy(
            src_ref=view, dst_ref=view, send_sem=z_send.at[k, d, hop - 1], recv_sem=z_recv.at[k, d, hop - 1],
            device_id={"fs": target}, device_id_type=MESH,
        )

    def x_copy(k, d, hop, s, half):
        view = chunks[k][0](s, half)
        return pltpu.make_async_remote_copy(
            src_ref=view, dst_ref=view, send_sem=x_send.at[k, d, hop - 1], recv_sem=x_recv.at[k, d, hop - 1],
            device_id={"rep": 1 - rep}, device_id_type=MESH,
        )

    pending = {}

    def z_send_start(step, k, d, hop, guard):
        s = here - (hop - 1) if d == 0 else here + (hop - 1)
        target = here + 1 if d == 0 else here - 1

        @pl.when(guard)
        def _():
            z_copy(k, d, hop, s, target).start()

        def finish():
            @pl.when(guard)
            def _():
                z_copy(k, d, hop, s, target).wait_send()

        pending.setdefault(step, []).append(finish)

    def own_send(step, k):
        for copy in chunks[k][1]:
            copy.wait()
        z_send_start(step, k, 0, 1, here <= 2)
        z_send_start(step, k, 1, 1, here >= 1)

    def arrive(step, k, d, hop):
        s = here - hop if d == 0 else here + hop
        origin = here - 1 if d == 0 else here + 1
        valid = here >= hop if d == 0 else here + hop <= 3

        @pl.when(valid)
        def _():
            z_copy(k, d, hop, s, origin).wait_recv()

        if hop < 3:
            onward = here <= 2 if d == 0 else here >= 1
            z_send_start(step, k, d, hop + 1, jnp.logical_and(valid, onward))

        @pl.when(valid)
        def _():
            x_copy(k, d, hop, s, rep).start()

        def finish():
            @pl.when(valid)
            def _():
                x_copy(k, d, hop, s, rep).wait_send()

        pending.setdefault(step, []).append(finish)

    def x_arrive(k, d, hop):
        s = here - hop if d == 0 else here + hop
        valid = here >= hop if d == 0 else here + hop <= 3

        @pl.when(valid)
        def _():
            x_copy(k, d, hop, s, 1 - rep).wait_recv()

    def finish_sends(step):
        for finish in pending.pop(step, ()):
            finish()

    def advance(step):
        finish_sends(step - 2)
        if step == 0:
            own_send(0, 0)
        if step + 1 < total:
            own_send(step, step + 1)
        for hop in (1, 2, 3):
            k = step - hop + 1
            if 0 <= k < total:
                for d in (0, 1):
                    arrive(step, k, d, hop)
        for hop in (1, 2, 3):
            k = step - hop
            if 0 <= k < total:
                for d in (0, 1):
                    x_arrive(k, d, hop)

    y_index = {}
    for name in ("gather1", "gather2", "reduce1"):
        for leg in ("beside", "across", "corner"):
            y_index[name, leg] = len(y_index) * seqs
    for leg in ("beside", "across", "corner"):
        y_index["reduce2", leg] = 9 * seqs + (len(y_index) - 9) * seqs * down_chunks

    def y_copy(name, leg, index, source, target, to):
        slot = y_index[name, leg] + index
        return pltpu.make_async_remote_copy(
            src_ref=source, dst_ref=target, send_sem=y_send.at[slot], recv_sem=y_recv.at[slot],
            device_id={"tp": to}, device_id_type=MESH,
        )

    def seq_rows(j):
        return pl.ds(j * SEQ, SEQ)

    def gather_copy(name, buffer, leg, j, arriving):
        to = across_id if leg == "across" else beside_id
        source_of = {"beside": (tp, beside_id), "across": (tp, across_id), "corner": (across_id, corner_id)}
        owner = source_of[leg][1 if arriving else 0]
        view = buffer.at[seq_rows(j), own_rows(width, owner)]
        return y_copy(name, leg, j, view, view, to)

    y_pending = []

    def gather_send(name, buffer, leg, j):
        copy = gather_copy(name, buffer, leg, j, False)
        copy.start()
        y_pending.append(copy)

    def gather_wait(name, buffer, leg, j):
        gather_copy(name, buffer, leg, j, True).wait_recv()

    def relay(name, buffer, j):
        gather_wait(name, buffer, "across", j)
        gather_send(name, buffer, "corner", j)

    def norm_into(source, gain_ref, target, source_row, target_row):
        group = 16

        @pl.loop(0, SEQ // group)
        def _(i):
            offset = pl.multiple_of(i * group, group)
            floats = source[pl.ds(source_row + offset, group), :].astype(f32)
            scale = lax.rsqrt(jnp.mean(floats * floats, axis=-1, keepdims=True) + epsilon)
            target[pl.ds(target_row + offset, group), :] = (floats * scale * gain_ref[...]).astype(bf16)

    def make_mask():
        gap = lax.broadcasted_iota(jnp.int32, (SEQ, SEQ), 0) - lax.broadcasted_iota(jnp.int32, (SEQ, SEQ), 1)
        positive = jnp.maximum(gap, 0).astype(f32)
        for head in range(heads):
            rate = rate_ref[pl.ds(tp * heads + head, 1), :]
            mask[head] = jnp.where(gap >= 0, jnp.exp(positive * rate), 0.0)

    def mix(j):
        gather_wait("gather1", x_all, "beside", j)
        gather_wait("gather1", x_all, "corner", j)
        norm_into(x_all, mix_gain_ref, normed, j * SEQ, 0)
        proj[...] = jnp.dot(normed[...], w_mix[...], preferred_element_type=f32).astype(bf16)
        highest = lax.Precision.HIGHEST
        lane = lax.broadcasted_iota(jnp.int32, (SEQ, key_width), 1)
        cosine, sine = cos_ref[...], sin_ref[...]

        def turn(values):
            following = pltpu.roll(values, key_width - 1, 1)
            preceding = pltpu.roll(values, 1, 1)
            other = jnp.where(lane % 2 == 0, -following, preceding)
            return values * cosine + other * sine

        query = turn(proj[:, :key_width].astype(f32))
        key = turn(proj[:, key_width : 2 * key_width].astype(f32)) * DK ** (-0.5)
        for head in range(heads):
            only = jnp.where(lane // DK == head, query, 0.0)
            scores = lax.dot_general(
                only, key, (((1,), (1,)), ((), ())), precision=highest, preferred_element_type=f32
            ) * mask[head]
            first = 2 * key_width + head * DV
            value = proj[:, first : first + DV].astype(f32)
            retained = jnp.dot(scores, value, precision=highest, preferred_element_type=f32)
            centered = retained - jnp.mean(retained, axis=-1, keepdims=True)
            spread = jnp.mean(centered * centered, axis=-1, keepdims=True)
            grouped = centered * lax.rsqrt(spread + epsilon) * head_gain_ref[head : head + 1, :]
            first += value_width
            gate = proj[:, first : first + DV].astype(f32)
            mixed[:, head * DV : (head + 1) * DV] = (grouped * jax.nn.silu(gate)).astype(bf16)

    def reduce_copy(name, leg, index, source, target):
        return y_copy(name, leg, index, source, target, across_id if leg == "across" else beside_id)

    def mix_reduce(j):
        def quarter(owner):
            return jnp.dot(mixed[...], w_out[:, own_rows(width, owner)], preferred_element_type=f32)

        def send(leg, source, target):
            copy = reduce_copy("reduce1", leg, j, source.at[j], target.at[j])
            copy.start()
            y_pending.append(copy)
            return copy

        corner1[j] = quarter(corner_id).astype(bf16)
        sent = send("corner", corner1, corner1_in)
        beside1[j] = quarter(beside_id).astype(bf16)
        send("beside", beside1, beside1_in)
        own1[j] = quarter(tp)
        far = quarter(across_id)
        sent.wait_recv()
        across1[j] = (far + corner1_in[j].astype(f32)).astype(bf16)
        send("across", across1, across1_in)

    def residual(j):
        reduce_copy("reduce1", "beside", j, beside1.at[j], beside1_in.at[j]).wait_recv()
        reduce_copy("reduce1", "across", j, across1.at[j], across1_in.at[j]).wait_recv()
        share = own1[j] + beside1_in[j].astype(f32) + across1_in[j].astype(f32)
        tokens = x_all[seq_rows(j), token_columns].astype(f32)
        res_all[seq_rows(j), token_columns] = (tokens + share).astype(bf16)
        gather_send("gather2", res_all, "across", j)
        gather_send("gather2", res_all, "beside", j)

    def ready(j):
        gather_wait("gather2", res_all, "beside", j)
        gather_wait("gather2", res_all, "corner", j)
        norm_into(res_all, ffn_gain_ref, normed_ffn, j * SEQ, j * SEQ)

    def ffn(first, last):
        @pl.loop(first, last)
        def _(b):
            weight_columns = own_rows(pair_width, b)
            hidden_columns = own_rows(LANES, b)

            @pl.loop(0, seqs)
            def _(j):
                part = own_rows(SEQ, j)
                both = jnp.dot(normed_ffn[part, :], w_ffn[:, weight_columns], preferred_element_type=f32)
                hidden[part, hidden_columns] = (jax.nn.silu(both[:, :LANES]) * both[:, LANES:]).astype(bf16)

    def reduce2(leg, c, j, source, target):
        part = own_rows(SEQ, j)
        return reduce_copy("reduce2", leg, c * seqs + j, source.at[c, part, :], target.at[c, part, :])

    def down(c):
        @pl.loop(0, seqs)
        def _(j):
            part = own_rows(SEQ, j)
            left = hidden[part, :]
            far = jnp.dot(left, w_down[c, :, own_rows(pair_width, 1 - chip)], preferred_element_type=f32)
            lower, upper = far[:, :LANES], far[:, LANES:]
            corner2[c, part, :] = jnp.where(core == 0, upper, lower).astype(bf16)
            sent = reduce2("corner", c, j, corner2, corner2_in)
            sent.start()
            onward = jnp.where(core == 0, lower, upper)
            near = jnp.dot(left, w_down[c, :, own_rows(pair_width, chip)], preferred_element_type=f32)
            lower, upper = near[:, :LANES], near[:, LANES:]
            beside2[c, part, :] = jnp.where(core == 0, upper, lower).astype(bf16)
            reduce2("beside", c, j, beside2, beside2_in).start()
            own2[c, part, :] = jnp.where(core == 0, lower, upper)
            sent.wait_recv()
            across2[c, part, :] = (onward + corner2_in[c, part, :].astype(f32)).astype(bf16)
            reduce2("across", c, j, across2, across2_in).start()

    def finish_down(c):
        @pl.loop(0, seqs)
        def _(j):
            part = own_rows(SEQ, j)
            reduce2("beside", c, j, beside2, beside2_in).wait_recv()
            reduce2("across", c, j, across2, across2_in).wait_recv()
            share = own2[c, part, :] + beside2_in[c, part, :].astype(f32) + across2_in[c, part, :].astype(f32)
            columns = pl.ds(pl.multiple_of(tp * width + c * LANES, LANES), LANES)
            kept = res_all[part, columns].astype(f32)
            out_ref[part, c * LANES : (c + 1) * LANES] = (kept + share).astype(bf16)
            for leg, source, target in (
                ("corner", corner2, corner2_in), ("beside", beside2, beside2_in), ("across", across2, across2_in),
            ):
                reduce2(leg, c, j, source, target).wait_send()

    work = {}

    def at(step, function, *args):
        work.setdefault(step, []).append((function, args))

    at(0, make_mask)
    for j in range(seqs):
        at(1 + j, relay, "gather1", x_all, j)
    mixed_at = mix_chunks + 2
    out_at = mixed_at + 1
    order = []
    for j in range(seqs):
        at(out_at + j + 3, ready, j)
    for j in range(seqs):
        at(out_at + j + 2, relay, "gather2", res_all, j)
    for j in range(seqs):
        at(out_at + j + 1, residual, j)
    for j in range(seqs):
        at(out_at + j, mix_reduce, j)
    for j in range(seqs):
        at(mixed_at + j, mix, j)
    done = 0
    ffn_from = out_at + seqs + 2
    for step in range(ffn_from, first_down + 3):
        there = min(ffn_blocks, step - first_ffn - 2)
        last = min(there, done + 4)
        if step == first_down + 2:
            last = ffn_blocks
        if last > done:
            at(step, ffn, done, last)
            done = last
    for c in range(down_chunks):
        at(first_down + 3 + c, down, c)
        if c:
            at(first_down + 3 + c, finish_down, c - 1)

    bring_tokens.wait()
    for j in range(seqs):
        gather_send("gather1", x_all, "across", j)
        gather_send("gather1", x_all, "beside", j)
    for step in range(total + 3):
        advance(step)
        for function, args in work.get(step, ()):
            function(*args)
    finish_down(down_chunks - 1)
    for step in sorted(pending):
        finish_sends(step)
    for copy in y_pending:
        copy.wait_send()


def layer(
    tokens, mix_gain, query_weight, key_weight, value_weight, gate_weight, out_weight, head_gain,
    ffn_gain, ffn_gate, ffn_up, ffn_down,
):
    bf16, f32 = jnp.bfloat16, jnp.float32
    rows, width = tokens.shape
    model = 4 * width
    seqs = rows // SEQ
    key_width, value_width = query_weight.shape[1], value_weight.shape[1]
    heads = head_gain.shape[0]
    mix_width = 2 * key_width + 2 * value_width
    hidden_width = ffn_gate.shape[1]
    blocks, down_chunks = hidden_width // LANES, ffn_down.shape[1] // LANES
    total = mix_width // (2 * LANES) + 1 + blocks + down_chunks
    frequency = rope_base ** (-np.linspace(0.0, 1.0, DK // 2))
    angles = np.arange(SEQ)[:, None] * frequency[None, :]
    cosine = np.tile(np.repeat(np.cos(angles), 2, axis=1), (1, heads)).astype(np.float32)
    sine = np.tile(np.repeat(np.sin(angles), 2, axis=1), (1, heads)).astype(np.float32)
    rates = np.log1p(-np.exp2(-5.0 - 4.0 * np.arange(HEADS) / (HEADS - 1)))
    rates = np.broadcast_to(rates[:, None], (HEADS, SEQ)).astype(np.float32)
    vmem, anywhere = pl.BlockSpec(memory_space=pltpu.VMEM), pl.BlockSpec(memory_space=pl.ANY)
    first_sum = [pltpu.VMEM((seqs, SEQ, width), bf16)] * 6
    second_sum = [pltpu.VMEM((down_chunks, rows, LANES), bf16)] * 6
    dma = pltpu.SemaphoreType.DMA
    return pl.pallas_call(
        fused_kernel,
        out_shape=jax.ShapeDtypeStruct((rows, width), bf16),
        in_specs=[anywhere, vmem] + [anywhere] * 5 + [vmem, vmem] + [anywhere] * 3 + [vmem] * 3,
        out_specs=vmem,
        scratch_shapes=[
            pltpu.VMEM((model, mix_width), bf16),
            pltpu.VMEM((out_weight.shape[0], model), bf16),
            pltpu.VMEM((model, 2 * hidden_width), bf16),
            pltpu.VMEM((down_chunks, hidden_width, 4 * LANES), bf16),
            pltpu.VMEM((rows, model), bf16),
            pltpu.VMEM((rows, model), bf16),
            pltpu.VMEM((SEQ, model), bf16),
            pltpu.VMEM((rows, model), bf16),
            pltpu.VMEM((SEQ, mix_width), bf16),
            pltpu.VMEM((SEQ, heads * DV), bf16),
            pltpu.VMEM((rows, hidden_width), bf16),
            pltpu.VMEM((heads, SEQ, SEQ), f32),
        ]
        + first_sum
        + [pltpu.VMEM((seqs, SEQ, width), f32)]
        + second_sum
        + [pltpu.VMEM((down_chunks, rows, LANES), f32)]
        + [
            dma((6 + 2 * blocks + down_chunks,)),
            dma((total, 2, 3)),
            dma((total, 2, 3)),
            dma((total, 2, 3)),
            dma((total, 2, 3)),
            dma((9 * seqs + 3 * seqs * down_chunks,)),
            dma((9 * seqs + 3 * seqs * down_chunks,)),
        ],
        compiler_params=pltpu.CompilerParams(
            collective_id=0, has_side_effects=True, vmem_limit_bytes=67043328
        ),
        name="layer",
    )(
        tokens, mix_gain.reshape(1, -1), query_weight, key_weight, value_weight, gate_weight, out_weight,
        head_gain, ffn_gain.reshape(1, -1), ffn_gate, ffn_up, ffn_down, cosine, sine, rates,
    )


def solution(mesh):
    shape = mesh.shape
    small = shape["rep"] == 2 and shape["fs"] == 4 and shape["tp"] == 4
    return jax.shard_map(
        layer if small else per_device_plain,
        mesh=mesh,
        in_specs=(
            P(("rep", "fs"), "tp"),
            P(),
            P("fs", "tp"),
            P("fs", "tp"),
            P("fs", "tp"),
            P("fs", "tp"),
            P("tp", "fs"),
            P("tp", None),
            P(),
            P("fs", "tp"),
            P("fs", "tp"),
            P("tp", "fs"),
        ),
        out_specs=P(("rep", "fs"), "tp"),
        check_vma=False,
    )
```

```python
import jax
import jax.numpy as jnp
import numpy as np
from jax import lax
from jax.experimental import pallas as pl
from jax.experimental.pallas import tpu as pltpu
from jax.sharding import PartitionSpec as P

HEADS = 8
DK = 64
DV = 128
BLOCK = 64
SEQ = 256


epsilon = 1e-06
rope_base = 10000.0


def norm_rows(values, gain_row):
    floats = values.astype(jnp.float32)
    scaled = floats * lax.rsqrt(jnp.mean(floats * floats, axis=-1, keepdims=True) + epsilon)
    return (scaled * gain_row).astype(jnp.bfloat16)


def rotate(values, positions):
    half_dim = values.shape[-1] // 2
    frequency = rope_base ** (-jnp.linspace(0.0, 1.0, half_dim, dtype=jnp.float32))
    angles = positions.astype(jnp.float32)[:, None] * frequency[None, :]
    cosine = jnp.cos(angles)[:, None, :]
    sine_part = jnp.sin(angles)[:, None, :]
    paired = values.reshape(values.shape[:-1] + (half_dim, 2))
    leading = paired[..., 0]
    trailing = paired[..., 1]
    turned = jnp.stack(
        [leading * cosine - trailing * sine_part, leading * sine_part + trailing * cosine], axis=-1
    )
    return turned.reshape(values.shape)


def log_decay(head_index, total_heads):
    return jnp.log1p(-jnp.exp2(-5.0 - 4.0 * head_index.astype(jnp.float32) / (total_heads - 1)))


def retention(queries, key_rows, value_rows, decay_rates):
    highest = lax.Precision.HIGHEST
    row_count, head_count = (queries.shape[0], queries.shape[1])
    seq_count = row_count // SEQ
    block_count = SEQ // BLOCK

    def to_blocks(values):
        shaped = values.reshape((seq_count, block_count, BLOCK) + values.shape[1:])
        return jnp.moveaxis(shaped, 1, 0)

    inside = jnp.arange(BLOCK, dtype=jnp.int32)
    gap = (inside[:, None] - inside[None, :]).astype(jnp.float32)
    within_mask = jnp.where(
        gap[None] >= 0.0, jnp.exp(jnp.maximum(gap, 0.0)[None] * decay_rates[:, None, None]), 0.0
    )
    query_scale = jnp.exp((inside + 1).astype(jnp.float32)[:, None] * decay_rates[None, :])
    key_scale = jnp.exp((BLOCK - 1 - inside).astype(jnp.float32)[:, None] * decay_rates[None, :])
    block_decay = jnp.exp(BLOCK * decay_rates)

    def advance(state, inputs):
        query_blk, key_blk, value_blk = inputs
        scores = (
            jnp.einsum("sihd,sjhd->shij", query_blk, key_blk, precision=highest) * within_mask[None]
        )
        local_part = jnp.einsum("shij,sjhv->sihv", scores, value_blk, precision=highest)
        carried = jnp.einsum(
            "sihd,shdv->sihv", query_blk * query_scale[None, :, :, None], state, precision=highest
        )
        update = jnp.einsum(
            "sjhd,sjhv->shdv", key_blk * key_scale[None, :, :, None], value_blk, precision=highest
        )
        return (block_decay[None, :, None, None] * state + update, local_part + carried)

    state_zero = jnp.zeros((seq_count, head_count, DK, DV), jnp.float32)
    _, outputs = lax.scan(
        advance, state_zero, (to_blocks(queries), to_blocks(key_rows), to_blocks(value_rows))
    )
    return jnp.moveaxis(outputs, 0, 1).reshape(row_count, head_count, DV)


def per_device_plain(
    tokens,
    mix_gain,
    query_weight,
    key_weight,
    value_weight,
    gate_weight,
    out_weight,
    head_gain,
    ffn_gain,
    ffn_gate,
    ffn_up,
    ffn_down,
):
    whole_rows = lax.all_gather(tokens, "tp", axis=1, tiled=True)
    row_count = whole_rows.shape[0]
    normed = norm_rows(whole_rows, mix_gain)
    pieces = (
        lax.all_gather(query_weight, "fs", axis=0, tiled=True),
        lax.all_gather(key_weight, "fs", axis=0, tiled=True),
        lax.all_gather(value_weight, "fs", axis=0, tiled=True),
        lax.all_gather(gate_weight, "fs", axis=0, tiled=True),
    )
    query_acc, key_acc, value_acc, gate_acc = tuple(
        (
            jnp.dot(normed, weight_piece, preferred_element_type=jnp.float32)
            for weight_piece in pieces
        )
    )
    heads_here = query_weight.shape[1] // DK
    positions = jnp.arange(row_count, dtype=jnp.int32) % SEQ
    queries = rotate(
        query_acc.astype(jnp.bfloat16).astype(jnp.float32).reshape(row_count, heads_here, DK),
        positions,
    )
    key_rows = rotate(
        key_acc.astype(jnp.bfloat16).astype(jnp.float32).reshape(row_count, heads_here, DK),
        positions,
    ) * DK ** (-0.5)
    value_rows = (
        value_acc.astype(jnp.bfloat16).astype(jnp.float32).reshape(row_count, heads_here, DV)
    )
    gate_rows = gate_acc.astype(jnp.bfloat16).astype(jnp.float32)
    first_head = lax.axis_index("tp") * heads_here
    decay_rates = log_decay(first_head + jnp.arange(heads_here, dtype=jnp.int32), HEADS)
    retained = retention(queries, key_rows, value_rows, decay_rates)
    center = jnp.mean(retained, axis=-1, keepdims=True)
    spread = jnp.mean(jnp.square(retained - center), axis=-1, keepdims=True)
    grouped = (retained - center) * lax.rsqrt(spread + epsilon) * head_gain[None]
    mixed = (grouped.reshape(row_count, heads_here * DV) * jax.nn.silu(gate_rows)).astype(
        jnp.bfloat16
    )
    mixer_terms = jnp.dot(
        mixed,
        lax.all_gather(out_weight, "fs", axis=1, tiled=True),
        preferred_element_type=jnp.float32,
    )
    mixer_share = lax.psum_scatter(
        mixer_terms.astype(jnp.bfloat16), "tp", scatter_dimension=1, tiled=True
    ).astype(jnp.float32)
    resid_shard = (tokens.astype(jnp.float32) + mixer_share).astype(jnp.bfloat16)
    resid_whole = lax.all_gather(resid_shard, "tp", axis=1, tiled=True)
    normed_ffn = norm_rows(resid_whole, ffn_gain)

    def add_rows(weight_piece):
        return jnp.dot(normed_ffn, weight_piece, preferred_element_type=jnp.float32)

    gate_hidden = add_rows(lax.all_gather(ffn_gate, "fs", axis=0, tiled=True))
    up_hidden = add_rows(lax.all_gather(ffn_up, "fs", axis=0, tiled=True))
    hidden = (jax.nn.silu(gate_hidden) * up_hidden).astype(jnp.bfloat16)
    ffn_terms = jnp.dot(
        hidden,
        lax.all_gather(ffn_down, "fs", axis=1, tiled=True),
        preferred_element_type=jnp.float32,
    )
    ffn_share = lax.psum_scatter(
        ffn_terms.astype(jnp.bfloat16), "tp", scatter_dimension=1, tiled=True
    ).astype(jnp.float32)
    return (resid_shard.astype(jnp.float32) + ffn_share).astype(jnp.bfloat16)


MESH = pl.DeviceIdType.MESH
LANES = 128
FFN_ROWS = 2
FFN_PER_STEP = 3
PLAN = ((0, 1, 3, 6, 10, 12), (2, 4, 5, 8, 14, 16), (5, 6, 7, 12, 18, 19), (8, 9, 11, 16, 20, 21))


def fused_kernel(
    tokens_ref, mix_gain_ref, query_ref, key_ref, value_ref, gate_ref, proj_out_ref, head_gain_ref,
    ffn_gain_ref, ffn_gate_ref, ffn_up_ref, ffn_down_ref, cos_ref, sin_ref, rate_ref,
    out_ref,
    w_mix, w_out, w_ffn, w_down, x_all, res_all, normed, normed_ffn, proj, mixed, hidden, mask,
    corner1, corner1_in, beside1, beside1_in, across1, across1_in, own1,
    corner2, corner2_in, beside2, beside2_in, across2, across2_in, own2, far2, sums, begun, result,
    local_sem, z_send, z_recv, x_send, x_recv, y_send, y_recv, out_sem,
):
    f32, bf16 = jnp.float32, jnp.bfloat16
    rep, here, tp = lax.axis_index("rep"), lax.axis_index("fs"), lax.axis_index("tp")
    core, chip = tp % 2, tp // 2
    beside_id, across_id, corner_id = tp + 1 - 2 * core, (tp + 2) % 4, 3 - tp
    rows, width = tokens_ref.shape
    seqs = rows // SEQ
    shard = query_ref.shape[0]
    key_width, value_width = query_ref.shape[1], value_ref.shape[1]
    heads = head_gain_ref.shape[0]
    ffn_blocks = ffn_gate_ref.shape[1] // LANES
    down_chunks = ffn_down_ref.shape[1] // LANES
    pair_width = 2 * LANES

    def own_rows(size, base=None):
        index = here if base is None else base
        return pl.ds(pl.multiple_of(index * size, size), size)

    def bring(slot, source, target):
        return pltpu.make_async_copy(source, target, local_sem.at[slot])

    token_columns = own_rows(width, tp)
    bring_tokens = bring(0, tokens_ref, x_all.at[:, token_columns])
    bring_mix = []
    start = 0
    for ref in (query_ref, key_ref, value_ref, gate_ref):
        bring_mix.append(bring(1 + len(bring_mix), ref, w_mix.at[own_rows(shard), pl.ds(start, ref.shape[1])]))
        start += ref.shape[1]
    bring_out = bring(5, proj_out_ref, w_out.at[:, own_rows(proj_out_ref.shape[1])])
    bring_ffn = [
        [
            bring(
                6 + 2 * (block % 4) + part,
                ref.at[:, pl.ds(block * LANES, LANES)],
                w_ffn.at[own_rows(shard), pl.ds(block * pair_width + part * LANES, LANES)],
            )
            for part, ref in enumerate((ffn_gate_ref, ffn_up_ref))
        ]
        for block in range(ffn_blocks)
    ]
    bring_down = [
        bring(14 + c, ffn_down_ref.at[:, pl.ds(c * LANES, LANES)], w_down.at[c, :, own_rows(LANES)])
        for c in range(down_chunks)
    ]

    chunks = []
    mix_chunks = w_mix.shape[1] // pair_width
    half_shard = shard // 2

    def row_chunk(buffer, column):
        def view(s, half):
            first = pl.multiple_of(s * shard + half * half_shard, half_shard)
            return buffer.at[pl.ds(first, half_shard), pl.ds(column, pair_width)]

        return view

    for i in range(mix_chunks):
        needs = {0: bring_mix[:2], 1: bring_mix[2:3], 2: bring_mix[3:]}[i]
        chunks.append((row_chunk(w_mix, i * pair_width), needs))

    def out_view(s, half):
        size, columns = w_out.shape[0] // 2, proj_out_ref.shape[1]
        return w_out.at[own_rows(size, half), own_rows(columns, s)]

    chunks.append((out_view, [bring_out]))
    for block in range(ffn_blocks):
        chunks.append((row_chunk(w_ffn, block * pair_width), bring_ffn[block]))

    def down_view(c, first, size):
        def view(s, half):
            rows_here = pl.ds(pl.multiple_of(first + half * (size // 2), LANES // 2), size // 2)
            return w_down.at[c, rows_here, own_rows(LANES, s)]

        return view

    hidden_width = w_down.shape[1]
    split = (ffn_blocks + 1) // 2 * LANES
    for c in range(down_chunks - 1):
        chunks.append((down_view(c, 0, hidden_width), [bring_down[c]]))
    chunks.append((down_view(down_chunks - 1, 0, split), [bring_down[-1]]))
    chunks.append((down_view(down_chunks - 1, split, hidden_width - split), []))
    total = len(chunks)
    first_ffn = mix_chunks + 1
    out_at_step = mix_chunks + 3
    first_down = first_ffn + ffn_blocks
    first_copies = 5

    for k in range(first_copies):
        if k == 1:
            bring_tokens.start()
        for copy in chunks[k][1]:
            copy.start()

    barrier = pltpu.get_barrier_semaphore()
    for target in (
        {"fs": (here + 1) % 4}, {"fs": (here + 3) % 4}, {"rep": 1 - rep}, {"tp": beside_id}, {"tp": across_id},
    ):
        pl.semaphore_signal(barrier, inc=1, device_id=target, device_id_type=MESH)
    pl.semaphore_wait(barrier, 5)

    def place(d, hop, receiver):
        return hop - 1 if d == 0 else receiver + hop - 1

    def z_copy(k, d, hop, s, target, receiver):
        view = chunks[k][0](s, rep)
        return pltpu.make_async_remote_copy(
            src_ref=view, dst_ref=view, send_sem=z_send.at[k % 3, d, hop - 1],
            recv_sem=z_recv.at[k, place(d, hop, receiver)], device_id={"fs": target}, device_id_type=MESH,
        )

    def extra_copy(k, d, target):
        view = chunks[k][0](here, 1 - rep)
        return pltpu.make_async_remote_copy(
            src_ref=view, dst_ref=view, send_sem=z_send.at[k % 3, d, 3],
            recv_sem=x_recv.at[k, place(d, 1, target)], device_id={"fs": target}, device_id_type=MESH,
        )

    def x_copy(k, d, hop, s, half):
        view = chunks[k][0](s, half)
        return pltpu.make_async_remote_copy(
            src_ref=view, dst_ref=view, send_sem=x_send.at[k % 3, d, hop - 1],
            recv_sem=x_recv.at[k, place(d, hop, here)], device_id={"rep": 1 - rep}, device_id_type=MESH,
        )

    pending = {}
    late = []
    at_end = jnp.logical_or(here == 0, here == 3)

    def guarded(step, guard, make):
        @pl.when(guard)
        def _():
            make().start()

        def finish():
            @pl.when(guard)
            def _():
                make().wait_send()

        pending.setdefault(step, []).append(finish)

    def z_send_start(step, k, d, hop, guard):
        s = here - (hop - 1) if d == 0 else here + (hop - 1)
        target = here + 1 if d == 0 else here - 1
        guarded(step, guard, lambda: z_copy(k, d, hop, s, target, target))

    def own_send(step, k):
        for copy in chunks[k][1]:
            copy.wait()
        z_send_start(step, k, 0, 1, here <= 2)
        z_send_start(step, k, 1, 1, here >= 1)

    def extra_send(step, k):
        guarded(step, here <= 1, lambda: extra_copy(k, 0, here + 1))
        guarded(step, here >= 2, lambda: extra_copy(k, 1, here - 1))

    def arrive(step, k, d, hop):
        s = here - hop if d == 0 else here + hop
        origin = here - 1 if d == 0 else here + 1
        valid = here >= hop if d == 0 else here + hop <= 3

        @pl.when(valid)
        def _():
            z_copy(k, d, hop, s, origin, here).wait_recv()

        if hop < 3:
            onward = here <= 2 if d == 0 else here >= 1
            z_send_start(step, k, d, hop + 1, jnp.logical_and(valid, onward))
        crosses = jnp.logical_and(valid, at_end) if hop == 1 else valid
        cross = lambda: guarded(step, crosses, lambda: x_copy(k, d, hop, s, rep))
        if k == total - 1 and hop < 3:
            late.append(cross)
        else:
            cross()

    def x_arrive(k, d, hop):
        s = here - hop if d == 0 else here + hop
        valid = here >= hop if d == 0 else here + hop <= 3

        @pl.when(valid)
        def _():
            x_copy(k, d, hop, s, 1 - rep).wait_recv()

    def finish_sends(step):
        for finish in pending.pop(step, ()):
            finish()

    def sent_at(k):
        return max(0, k - 1 if k <= out_at_step else k - 2)

    def advance(step, hop):
        if hop == 1:
            finish_sends(step - 2)
            for k in range(total):
                if sent_at(k) == step:
                    own_send(step, k)
            if step + first_copies < total:
                for copy in chunks[step + first_copies][1]:
                    copy.start()
        k = step - hop + 1
        if 0 <= k < total:
            for d in (0, 1):
                arrive(step, k, d, hop)
        if hop == 1 and 0 <= step - 1 < total:
            extra_send(step, step - 1)
        if hop == 3:
            while late:
                late.pop(0)()
        if hop == 3 and 0 <= step - 3 < total:
            for leg in (1, 2, 3):
                for d in (0, 1):
                    x_arrive(step - 3, d, leg)

    y_index = {}
    for name in ("gather1", "gather2", "reduce1"):
        for leg in ("beside", "across", "corner"):
            y_index[name, leg] = len(y_index) * seqs
    for leg in ("beside", "across", "corner"):
        y_index["reduce2", leg] = 9 * seqs + (len(y_index) - 9) * seqs * down_chunks

    send_group = {"gather1": 0, "gather2": 0, "reduce1": 1, "reduce2": 2}
    legs = ("beside", "across", "corner")

    def y_copy(name, leg, index, source, target, to, send_index=None):
        group = send_group[name] * 3 * seqs + legs.index(leg) * (2 * seqs if name == "reduce2" else seqs)
        return pltpu.make_async_remote_copy(
            src_ref=source, dst_ref=target,
            send_sem=y_send.at[group + (index if send_index is None else send_index)],
            recv_sem=y_recv.at[y_index[name, leg] + index], device_id={"tp": to}, device_id_type=MESH,
        )

    def seq_rows(j):
        return pl.ds(j * SEQ, SEQ)

    def gather_copy(name, buffer, leg, j, arriving):
        to = across_id if leg == "across" else beside_id
        source_of = {"beside": (tp, beside_id), "across": (tp, across_id), "corner": (across_id, corner_id)}
        owner = source_of[leg][1 if arriving else 0]
        view = buffer.at[seq_rows(j), own_rows(width, owner)]
        return y_copy(name, leg, j, view, view, to)

    y_pending = []

    def gather_send(name, buffer, leg, j):
        copy = gather_copy(name, buffer, leg, j, False)
        copy.start()
        y_pending.append(copy)

    def gather_wait(name, buffer, leg, j):
        gather_copy(name, buffer, leg, j, True).wait_recv()

    def relay(name, buffer, j):
        gather_wait(name, buffer, "across", j)
        gather_send(name, buffer, "corner", j)

    def norm_into(source, gain_ref, target, source_row, target_row):
        group = 16

        @pl.loop(0, SEQ // group, unroll=4)
        def _(i):
            offset = pl.multiple_of(i * group, group)
            floats = source[pl.ds(source_row + offset, group), :].astype(f32)
            scale = lax.rsqrt(jnp.mean(floats * floats, axis=-1, keepdims=True) + epsilon)
            target[pl.ds(target_row + offset, group), :] = (floats * scale * gain_ref[...]).astype(bf16)

    def make_mask():
        gap = lax.broadcasted_iota(jnp.int32, (SEQ, SEQ), 0) - lax.broadcasted_iota(jnp.int32, (SEQ, SEQ), 1)
        positive = jnp.maximum(gap, 0).astype(f32)
        for head in range(heads):
            rate = rate_ref[pl.ds(tp * heads + head, 1), :]
            mask[head] = jnp.where(gap >= 0, jnp.exp(positive * rate), 0.0)

    def project(j):
        gather_wait("gather1", x_all, "beside", j)
        gather_wait("gather1", x_all, "corner", j)
        norm_into(x_all, mix_gain_ref, normed, j * SEQ, 0)
        proj[...] = jnp.dot(normed[...], w_mix[...], preferred_element_type=f32).astype(bf16)

    def retain():
        highest = lax.Precision.HIGHEST
        lane = lax.broadcasted_iota(jnp.int32, (SEQ, key_width), 1)
        cosine, sine = cos_ref[...], sin_ref[...]

        def turn(values):
            following = pltpu.roll(values, key_width - 1, 1)
            preceding = pltpu.roll(values, 1, 1)
            other = jnp.where(lane % 2 == 0, -following, preceding)
            return values * cosine + other * sine

        query = turn(proj[:, :key_width].astype(f32))
        key = turn(proj[:, key_width : 2 * key_width].astype(f32)) * DK ** (-0.5)
        for head in range(heads):
            only = jnp.where(lane // DK == head, query, 0.0)
            scores = lax.dot_general(
                only, key, (((1,), (1,)), ((), ())), precision=highest, preferred_element_type=f32
            ) * mask[head]
            first = 2 * key_width + head * DV
            value = proj[:, first : first + DV].astype(f32)
            retained = jnp.dot(scores, value, precision=highest, preferred_element_type=f32)
            centered = retained - jnp.mean(retained, axis=-1, keepdims=True)
            spread = jnp.mean(centered * centered, axis=-1, keepdims=True)
            grouped = centered * lax.rsqrt(spread + epsilon) * head_gain_ref[head : head + 1, :]
            first += value_width
            gate = proj[:, first : first + DV].astype(f32)
            mixed[:, head * DV : (head + 1) * DV] = (grouped * jax.nn.silu(gate)).astype(bf16)

    def reduce_copy(name, leg, index, source, target, send_index=None):
        to = across_id if leg == "across" else beside_id
        return y_copy(name, leg, index, source, target, to, send_index)

    def mix_reduce(j):
        def quarter(owner):
            return jnp.dot(mixed[...], w_out[:, own_rows(width, owner)], preferred_element_type=f32)

        def send(leg, source, target):
            copy = reduce_copy("reduce1", leg, j, source.at[j], target.at[j])
            copy.start()
            y_pending.append(copy)
            return copy

        corner1[j] = quarter(corner_id).astype(bf16)
        sent = send("corner", corner1, corner1_in)
        beside1[j] = quarter(beside_id).astype(bf16)
        send("beside", beside1, beside1_in)
        own1[j] = quarter(tp)
        far = quarter(across_id)
        sent.wait_recv()
        across1[j] = (far + corner1_in[j].astype(f32)).astype(bf16)
        send("across", across1, across1_in)

    def residual(j):
        reduce_copy("reduce1", "beside", j, beside1.at[j], beside1_in.at[j]).wait_recv()
        reduce_copy("reduce1", "across", j, across1.at[j], across1_in.at[j]).wait_recv()
        share = own1[j] + beside1_in[j].astype(f32) + across1_in[j].astype(f32)
        tokens = x_all[seq_rows(j), token_columns].astype(f32)
        res_all[seq_rows(j), token_columns] = (tokens + share).astype(bf16)
        gather_send("gather2", res_all, "across", j)
        gather_send("gather2", res_all, "beside", j)

    def ready(j):
        gather_wait("gather2", res_all, "beside", j)
        gather_wait("gather2", res_all, "corner", j)
        norm_into(res_all, ffn_gain_ref, normed_ffn, j * SEQ, j * SEQ)

    def ffn(b):
        group = FFN_ROWS * SEQ
        weight = w_ffn.at[:, pl.ds(b * pair_width, pair_width)]

        @pl.loop(0, rows // group)
        def _(j):
            part = own_rows(group, j)
            both = jnp.dot(normed_ffn[part, :], weight[...], preferred_element_type=f32)
            hidden[part, b * LANES : (b + 1) * LANES] = (
                jax.nn.silu(both[:, :LANES]) * both[:, LANES:]
            ).astype(bf16)

    def reduce2(leg, c, j, source, target):
        part = own_rows(SEQ, j)
        slot = (c % 2) * seqs + j
        return reduce_copy("reduce2", leg, c * seqs + j, source.at[c, part, :], target.at[c, part, :], slot)

    def down_products(c, j):
        part = own_rows(SEQ, j)
        if c + 1 < down_chunks:
            sums[...] = jnp.dot(hidden[part, :], w_down[c], preferred_element_type=f32)
        else:
            sums[...] = begun[part, :] + jnp.dot(
                hidden[part, split:], w_down[c, split:, :], preferred_element_type=f32
            )
        corner2[c, part, :] = sums[:, own_rows(LANES, corner_id)].astype(bf16)
        reduce2("corner", c, j, corner2, corner2_in).start()
        beside2[c, part, :] = sums[:, own_rows(LANES, beside_id)].astype(bf16)
        reduce2("beside", c, j, beside2, beside2_in).start()
        far2[part, :] = sums[:, own_rows(LANES, across_id)]
        own2[c, part, :] = sums[:, own_rows(LANES, tp)]

    def down_begin(c):
        @pl.loop(0, seqs)
        def _(j):
            part = own_rows(SEQ, j)
            begun[part, :] = jnp.dot(hidden[part, :split], w_down[c, :split, :], preferred_element_type=f32)

    def down_onward(c, j):
        part = own_rows(SEQ, j)
        reduce2("corner", c, j, corner2, corner2_in).wait_recv()
        across2[c, part, :] = (far2[part, :] + corner2_in[c, part, :].astype(f32)).astype(bf16)
        reduce2("across", c, j, across2, across2_in).start()

    def down(c):
        @pl.loop(0, seqs)
        def _(j):
            down_products(c, j)

    def down_rest(c):
        @pl.loop(0, seqs)
        def _(j):
            down_onward(c, j)

    def down_last(c):
        @pl.loop(0, seqs + 1)
        def _(j):
            @pl.when(j < seqs)
            def _():
                down_products(c, j)

            @pl.when(j > 0)
            def _():
                down_onward(c, j - 1)

    def finish_down(c):
        @pl.loop(0, seqs)
        def _(j):
            part = own_rows(SEQ, j)
            reduce2("beside", c, j, beside2, beside2_in).wait_recv()
            reduce2("across", c, j, across2, across2_in).wait_recv()
            share = own2[c, part, :] + beside2_in[c, part, :].astype(f32) + across2_in[c, part, :].astype(f32)
            columns = pl.ds(pl.multiple_of(tp * width + c * LANES, LANES), LANES)
            kept = res_all[part, columns].astype(f32)
            result[c, part, :] = (kept + share).astype(bf16)
            for leg, source, target in (
                ("corner", corner2, corner2_in), ("beside", beside2, beside2_in), ("across", across2, across2_in),
            ):
                reduce2(leg, c, j, source, target).wait_send()

        out_copy(c).start()

    def out_copy(c):
        return pltpu.make_async_copy(result.at[c], out_ref.at[:, pl.ds(c * LANES, LANES)], out_sem.at[c])

    work = {}

    def at(slot, function, *args):
        work.setdefault(slot, []).append((function, args))

    at(0, make_mask)
    for j in range(seqs):
        at(5 + 3 * j, relay, "gather1", x_all, j)
    base = 3 * (mix_chunks + 2) + 2
    for j, (a, b, r, s, l, n) in enumerate(PLAN):
        at(base + s, residual, j)
        at(base + l, relay, "gather2", res_all, j)
        at(base + n, ready, j)
        at(base + b, retain)
        at(base + r, mix_reduce, j)
        at(base + a, project, j)
    def finish_gather():
        for copy in y_pending[: 3 * seqs]:
            copy.wait_send()
        del y_pending[: 3 * seqs]

    at(base + min(r for _, _, r, *_ in PLAN), finish_gather)
    slot = base + 1 + max(n for *_, n in PLAN)
    for block in range(ffn_blocks):
        slot = max(slot, 3 * (first_ffn + block + 3) + 2)
        at(slot, ffn, block)
        slot += 1 if slot % 3 != FFN_PER_STEP - 1 else 4 - FFN_PER_STEP
    for c in range(down_chunks - 1):
        complete = 3 * (first_down + 3 + c) + 2
        if c + 2 < down_chunks:
            at(complete, down, c)
            at(complete + 1, down_rest, c)
        else:
            at(complete, down_last, c)
        if c + 2 < down_chunks:
            at(complete + 5, finish_down, c)
    last_slot = 3 * (total + 3) - 1
    at(last_slot - 3, down_begin, down_chunks - 1)

    bring_tokens.wait()
    for j in range(seqs):
        gather_send("gather1", x_all, "across", j)
        gather_send("gather1", x_all, "beside", j)
    for slot in range(3 * (total + 3)):
        advance(slot // 3, slot % 3 + 1)
        for function, args in work.get(slot, ()):
            function(*args)
    down_last(down_chunks - 1)
    finish_down(down_chunks - 2)
    finish_down(down_chunks - 1)
    for step in sorted(pending):
        finish_sends(step)
    for copy in y_pending:
        copy.wait_send()
    for c in range(down_chunks):
        out_copy(c).wait()


def layer(
    tokens, mix_gain, query_weight, key_weight, value_weight, gate_weight, out_weight, head_gain,
    ffn_gain, ffn_gate, ffn_up, ffn_down,
):
    bf16, f32 = jnp.bfloat16, jnp.float32
    rows, width = tokens.shape
    model = 4 * width
    seqs = rows // SEQ
    key_width, value_width = query_weight.shape[1], value_weight.shape[1]
    heads = head_gain.shape[0]
    mix_width = 2 * key_width + 2 * value_width
    hidden_width = ffn_gate.shape[1]
    blocks, down_chunks = hidden_width // LANES, ffn_down.shape[1] // LANES
    total = mix_width // (2 * LANES) + 1 + blocks + down_chunks + 1
    frequency = rope_base ** (-np.linspace(0.0, 1.0, DK // 2))
    angles = np.arange(SEQ)[:, None] * frequency[None, :]
    cosine = np.tile(np.repeat(np.cos(angles), 2, axis=1), (1, heads)).astype(np.float32)
    sine = np.tile(np.repeat(np.sin(angles), 2, axis=1), (1, heads)).astype(np.float32)
    rates = np.log1p(-np.exp2(-5.0 - 4.0 * np.arange(HEADS) / (HEADS - 1)))
    rates = np.broadcast_to(rates[:, None], (HEADS, SEQ)).astype(np.float32)
    vmem, anywhere = pl.BlockSpec(memory_space=pltpu.VMEM), pl.BlockSpec(memory_space=pl.ANY)
    first_sum = [pltpu.VMEM((seqs, SEQ, width), bf16)] * 6
    second_sum = [pltpu.VMEM((down_chunks, rows, LANES), bf16)] * 6
    dma = pltpu.SemaphoreType.DMA
    return pl.pallas_call(
        fused_kernel,
        out_shape=jax.ShapeDtypeStruct((rows, width), bf16),
        in_specs=[anywhere, vmem] + [anywhere] * 5 + [vmem, vmem] + [anywhere] * 3 + [vmem] * 3,
        out_specs=anywhere,
        scratch_shapes=[
            pltpu.VMEM((model, mix_width), bf16),
            pltpu.VMEM((out_weight.shape[0], model), bf16),
            pltpu.VMEM((model, 2 * hidden_width), bf16),
            pltpu.VMEM((down_chunks, hidden_width, 4 * LANES), bf16),
            pltpu.VMEM((rows, model), bf16),
            pltpu.VMEM((rows, model), bf16),
            pltpu.VMEM((SEQ, model), bf16),
            pltpu.VMEM((rows, model), bf16),
            pltpu.VMEM((SEQ, mix_width), bf16),
            pltpu.VMEM((SEQ, heads * DV), bf16),
            pltpu.VMEM((rows, hidden_width), bf16),
            pltpu.VMEM((heads, SEQ, SEQ), f32),
        ]
        + first_sum
        + [pltpu.VMEM((seqs, SEQ, width), f32)]
        + second_sum
        + [
            pltpu.VMEM((down_chunks, rows, LANES), f32),
            pltpu.VMEM((rows, LANES), f32),
            pltpu.VMEM((SEQ, 4 * LANES), f32),
            pltpu.VMEM((rows, 4 * LANES), f32),
            pltpu.VMEM((down_chunks, rows, LANES), bf16),
        ]
        + [
            dma((14 + down_chunks,)),
            dma((3, 2, 4)),
            dma((total, 3)),
            dma((3, 2, 3)),
            dma((total, 3)),
            dma((12 * seqs,)),
            dma((9 * seqs + 3 * seqs * down_chunks,)),
            dma((down_chunks,)),
        ],
        compiler_params=pltpu.CompilerParams(
            collective_id=0, has_side_effects=True, vmem_limit_bytes=67043328
        ),
        name="layer",
    )(
        tokens, mix_gain.reshape(1, -1), query_weight, key_weight, value_weight, gate_weight, out_weight,
        head_gain, ffn_gain.reshape(1, -1), ffn_gate, ffn_up, ffn_down, cosine, sine, rates,
    )


def solution(mesh):
    shape = mesh.shape
    small = shape["rep"] == 2 and shape["fs"] == 4 and shape["tp"] == 4
    return jax.shard_map(
        layer if small else per_device_plain,
        mesh=mesh,
        in_specs=(
            P(("rep", "fs"), "tp"),
            P(),
            P("fs", "tp"),
            P("fs", "tp"),
            P("fs", "tp"),
            P("fs", "tp"),
            P("tp", "fs"),
            P("tp", None),
            P(),
            P("fs", "tp"),
            P("fs", "tp"),
            P("tp", "fs"),
        ),
        out_specs=P(("rep", "fs"), "tp"),
        check_vma=False,
    )
```

```python
import jax
import jax.numpy as jnp
import numpy as np
from jax import lax
from jax.experimental import pallas as pl
from jax.experimental.pallas import tpu as pltpu
from jax.sharding import PartitionSpec as P

HEADS = 8
DK = 64
DV = 128
BLOCK = 64
SEQ = 256


epsilon = 1e-06
rope_base = 10000.0


def norm_rows(values, gain_row):
    floats = values.astype(jnp.float32)
    scaled = floats * lax.rsqrt(jnp.mean(floats * floats, axis=-1, keepdims=True) + epsilon)
    return (scaled * gain_row).astype(jnp.bfloat16)


def rotate(values, positions):
    half_dim = values.shape[-1] // 2
    frequency = rope_base ** (-jnp.linspace(0.0, 1.0, half_dim, dtype=jnp.float32))
    angles = positions.astype(jnp.float32)[:, None] * frequency[None, :]
    cosine = jnp.cos(angles)[:, None, :]
    sine_part = jnp.sin(angles)[:, None, :]
    paired = values.reshape(values.shape[:-1] + (half_dim, 2))
    leading = paired[..., 0]
    trailing = paired[..., 1]
    turned = jnp.stack(
        [leading * cosine - trailing * sine_part, leading * sine_part + trailing * cosine], axis=-1
    )
    return turned.reshape(values.shape)


def log_decay(head_index, total_heads):
    return jnp.log1p(-jnp.exp2(-5.0 - 4.0 * head_index.astype(jnp.float32) / (total_heads - 1)))


def retention(queries, key_rows, value_rows, decay_rates):
    highest = lax.Precision.HIGHEST
    row_count, head_count = (queries.shape[0], queries.shape[1])
    seq_count = row_count // SEQ
    block_count = SEQ // BLOCK

    def to_blocks(values):
        shaped = values.reshape((seq_count, block_count, BLOCK) + values.shape[1:])
        return jnp.moveaxis(shaped, 1, 0)

    inside = jnp.arange(BLOCK, dtype=jnp.int32)
    gap = (inside[:, None] - inside[None, :]).astype(jnp.float32)
    within_mask = jnp.where(
        gap[None] >= 0.0, jnp.exp(jnp.maximum(gap, 0.0)[None] * decay_rates[:, None, None]), 0.0
    )
    query_scale = jnp.exp((inside + 1).astype(jnp.float32)[:, None] * decay_rates[None, :])
    key_scale = jnp.exp((BLOCK - 1 - inside).astype(jnp.float32)[:, None] * decay_rates[None, :])
    block_decay = jnp.exp(BLOCK * decay_rates)

    def advance(state, inputs):
        query_blk, key_blk, value_blk = inputs
        scores = (
            jnp.einsum("sihd,sjhd->shij", query_blk, key_blk, precision=highest) * within_mask[None]
        )
        local_part = jnp.einsum("shij,sjhv->sihv", scores, value_blk, precision=highest)
        carried = jnp.einsum(
            "sihd,shdv->sihv", query_blk * query_scale[None, :, :, None], state, precision=highest
        )
        update = jnp.einsum(
            "sjhd,sjhv->shdv", key_blk * key_scale[None, :, :, None], value_blk, precision=highest
        )
        return (block_decay[None, :, None, None] * state + update, local_part + carried)

    state_zero = jnp.zeros((seq_count, head_count, DK, DV), jnp.float32)
    _, outputs = lax.scan(
        advance, state_zero, (to_blocks(queries), to_blocks(key_rows), to_blocks(value_rows))
    )
    return jnp.moveaxis(outputs, 0, 1).reshape(row_count, head_count, DV)


def per_device_plain(
    tokens,
    mix_gain,
    query_weight,
    key_weight,
    value_weight,
    gate_weight,
    out_weight,
    head_gain,
    ffn_gain,
    ffn_gate,
    ffn_up,
    ffn_down,
):
    whole_rows = lax.all_gather(tokens, "tp", axis=1, tiled=True)
    row_count = whole_rows.shape[0]
    normed = norm_rows(whole_rows, mix_gain)
    pieces = (
        lax.all_gather(query_weight, "fs", axis=0, tiled=True),
        lax.all_gather(key_weight, "fs", axis=0, tiled=True),
        lax.all_gather(value_weight, "fs", axis=0, tiled=True),
        lax.all_gather(gate_weight, "fs", axis=0, tiled=True),
    )
    query_acc, key_acc, value_acc, gate_acc = tuple(
        (
            jnp.dot(normed, weight_piece, preferred_element_type=jnp.float32)
            for weight_piece in pieces
        )
    )
    heads_here = query_weight.shape[1] // DK
    positions = jnp.arange(row_count, dtype=jnp.int32) % SEQ
    queries = rotate(
        query_acc.astype(jnp.bfloat16).astype(jnp.float32).reshape(row_count, heads_here, DK),
        positions,
    )
    key_rows = rotate(
        key_acc.astype(jnp.bfloat16).astype(jnp.float32).reshape(row_count, heads_here, DK),
        positions,
    ) * DK ** (-0.5)
    value_rows = (
        value_acc.astype(jnp.bfloat16).astype(jnp.float32).reshape(row_count, heads_here, DV)
    )
    gate_rows = gate_acc.astype(jnp.bfloat16).astype(jnp.float32)
    first_head = lax.axis_index("tp") * heads_here
    decay_rates = log_decay(first_head + jnp.arange(heads_here, dtype=jnp.int32), HEADS)
    retained = retention(queries, key_rows, value_rows, decay_rates)
    center = jnp.mean(retained, axis=-1, keepdims=True)
    spread = jnp.mean(jnp.square(retained - center), axis=-1, keepdims=True)
    grouped = (retained - center) * lax.rsqrt(spread + epsilon) * head_gain[None]
    mixed = (grouped.reshape(row_count, heads_here * DV) * jax.nn.silu(gate_rows)).astype(
        jnp.bfloat16
    )
    mixer_terms = jnp.dot(
        mixed,
        lax.all_gather(out_weight, "fs", axis=1, tiled=True),
        preferred_element_type=jnp.float32,
    )
    mixer_share = lax.psum_scatter(
        mixer_terms.astype(jnp.bfloat16), "tp", scatter_dimension=1, tiled=True
    ).astype(jnp.float32)
    resid_shard = (tokens.astype(jnp.float32) + mixer_share).astype(jnp.bfloat16)
    resid_whole = lax.all_gather(resid_shard, "tp", axis=1, tiled=True)
    normed_ffn = norm_rows(resid_whole, ffn_gain)

    def add_rows(weight_piece):
        return jnp.dot(normed_ffn, weight_piece, preferred_element_type=jnp.float32)

    gate_hidden = add_rows(lax.all_gather(ffn_gate, "fs", axis=0, tiled=True))
    up_hidden = add_rows(lax.all_gather(ffn_up, "fs", axis=0, tiled=True))
    hidden = (jax.nn.silu(gate_hidden) * up_hidden).astype(jnp.bfloat16)
    ffn_terms = jnp.dot(
        hidden,
        lax.all_gather(ffn_down, "fs", axis=1, tiled=True),
        preferred_element_type=jnp.float32,
    )
    ffn_share = lax.psum_scatter(
        ffn_terms.astype(jnp.bfloat16), "tp", scatter_dimension=1, tiled=True
    ).astype(jnp.float32)
    return (resid_shard.astype(jnp.float32) + ffn_share).astype(jnp.bfloat16)


MESH = pl.DeviceIdType.MESH
LANES = 128
FFN_ROWS = 2
FFN_PER_STEP = 3
PLAN = ((0, 1, 3, 6, 10, 12), (2, 4, 5, 8, 14, 16), (5, 6, 7, 12, 19, 20), (8, 9, 11, 17, 21, 22))


def fused_kernel(
    tokens_ref, mix_gain_hbm, query_ref, key_ref, value_ref, gate_ref, proj_out_ref, head_gain_hbm,
    ffn_gain_hbm, ffn_gate_ref, ffn_up_ref, ffn_down_ref, cos_hbm, sin_hbm, rate_hbm,
    out_ref,
    mix_gain_ref, head_gain_ref, ffn_gain_ref, cos_ref, sin_ref, rate_ref,
    w_mix, w_out, w_ffn, w_down, x_all, res_all, normed, normed_ffn, proj, mixed, hidden, mask,
    corner1, corner1_in, beside1, beside1_in, across1, across1_in, own1,
    corner2, corner2_in, beside2, beside2_in, across2, across2_in, own2, far2, sums, begun, result,
    local_sem, z_send, z_recv, x_send, x_recv, y_send, y_recv, out_sem,
):
    f32, bf16 = jnp.float32, jnp.bfloat16
    rep, here, tp = lax.axis_index("rep"), lax.axis_index("fs"), lax.axis_index("tp")
    core, chip = tp % 2, tp // 2
    beside_id, across_id, corner_id = tp + 1 - 2 * core, (tp + 2) % 4, 3 - tp
    rows, width = tokens_ref.shape
    seqs = rows // SEQ
    shard = query_ref.shape[0]
    key_width, value_width = query_ref.shape[1], value_ref.shape[1]
    heads = head_gain_ref.shape[0]
    ffn_blocks = ffn_gate_ref.shape[1] // LANES
    down_chunks = ffn_down_ref.shape[1] // LANES
    pair_width = 2 * LANES

    def own_rows(size, base=None):
        index = here if base is None else base
        return pl.ds(pl.multiple_of(index * size, size), size)

    barrier = pltpu.get_barrier_semaphore()
    for target in (
        {"fs": (here + 1) % 4}, {"fs": (here + 3) % 4}, {"rep": 1 - rep}, {"tp": beside_id}, {"tp": across_id},
    ):
        pl.semaphore_signal(barrier, inc=1, device_id=target, device_id_type=MESH)

    def bring(slot, source, target):
        return pltpu.make_async_copy(source, target, local_sem.at[slot])

    token_columns = own_rows(width, tp)
    bring_tokens = bring(0, tokens_ref, x_all.at[:, token_columns])
    bring_mix = []
    start = 0
    for ref in (query_ref, key_ref, value_ref, gate_ref):
        bring_mix.append(bring(1 + len(bring_mix), ref, w_mix.at[own_rows(shard), pl.ds(start, ref.shape[1])]))
        start += ref.shape[1]
    bring_out = bring(5, proj_out_ref, w_out.at[:, own_rows(proj_out_ref.shape[1])])
    bring_ffn = [
        [
            bring(
                6 + 2 * (block % 4) + part,
                ref.at[:, pl.ds(block * LANES, LANES)],
                w_ffn.at[own_rows(shard), pl.ds(block * pair_width + part * LANES, LANES)],
            )
            for part, ref in enumerate((ffn_gate_ref, ffn_up_ref))
        ]
        for block in range(ffn_blocks)
    ]
    bring_down = [
        bring(14 + c, ffn_down_ref.at[:, pl.ds(c * LANES, LANES)], w_down.at[c, :, own_rows(LANES)])
        for c in range(down_chunks)
    ]

    chunks = []
    mix_chunks = w_mix.shape[1] // pair_width
    half_shard = shard // 2

    def row_chunk(buffer, column):
        def view(s, half):
            first = pl.multiple_of(s * shard + half * half_shard, half_shard)
            return buffer.at[pl.ds(first, half_shard), pl.ds(column, pair_width)]

        return view

    for i in range(mix_chunks):
        needs = {0: bring_mix[:2], 1: bring_mix[2:3], 2: bring_mix[3:]}[i]
        chunks.append((row_chunk(w_mix, i * pair_width), needs))

    def out_view(s, half):
        size, columns = w_out.shape[0] // 2, proj_out_ref.shape[1]
        return w_out.at[own_rows(size, half), own_rows(columns, s)]

    chunks.append((out_view, [bring_out]))
    for block in range(ffn_blocks):
        chunks.append((row_chunk(w_ffn, block * pair_width), bring_ffn[block]))

    def down_view(c, first, size):
        def view(s, half):
            rows_here = pl.ds(pl.multiple_of(first + half * (size // 2), LANES // 2), size // 2)
            return w_down.at[c, rows_here, own_rows(LANES, s)]

        return view

    hidden_width = w_down.shape[1]
    split = (ffn_blocks + 1) // 2 * LANES
    for c in range(down_chunks - 1):
        chunks.append((down_view(c, 0, hidden_width), [bring_down[c]]))
    chunks.append((down_view(down_chunks - 1, 0, split), [bring_down[-1]]))
    chunks.append((down_view(down_chunks - 1, split, hidden_width - split), []))
    total = len(chunks)
    first_ffn = mix_chunks + 1
    first_down = first_ffn + ffn_blocks
    first_copies = 5

    for k in range(first_copies):
        if k == 1:
            bring_tokens.start()
        for copy in chunks[k][1]:
            copy.start()
    bring_small = [
        bring(14 + down_chunks + i, source, target)
        for i, (source, target) in enumerate(
            (
                (mix_gain_hbm, mix_gain_ref), (head_gain_hbm, head_gain_ref), (ffn_gain_hbm, ffn_gain_ref),
                (cos_hbm, cos_ref), (sin_hbm, sin_ref), (rate_hbm, rate_ref),
            )
        )
    ]
    for copy in bring_small:
        copy.start()
    pl.semaphore_wait(barrier, 5)

    def place(d, hop, receiver):
        return hop - 1 if d == 0 else receiver + hop - 1

    def z_copy(k, d, hop, s, target, receiver):
        view = chunks[k][0](s, rep)
        return pltpu.make_async_remote_copy(
            src_ref=view, dst_ref=view, send_sem=z_send.at[k % 3, d, hop - 1],
            recv_sem=z_recv.at[k, place(d, hop, receiver)], device_id={"fs": target}, device_id_type=MESH,
        )

    def extra_copy(k, d, target):
        view = chunks[k][0](here, 1 - rep)
        return pltpu.make_async_remote_copy(
            src_ref=view, dst_ref=view, send_sem=z_send.at[k % 3, d, 3],
            recv_sem=x_recv.at[k, place(d, 1, target)], device_id={"fs": target}, device_id_type=MESH,
        )

    def x_copy(k, d, hop, s, half):
        view = chunks[k][0](s, half)
        return pltpu.make_async_remote_copy(
            src_ref=view, dst_ref=view, send_sem=x_send.at[k % 3, d, hop - 1],
            recv_sem=x_recv.at[k, place(d, hop, here)], device_id={"rep": 1 - rep}, device_id_type=MESH,
        )

    pending = {}
    late = []
    at_end = jnp.logical_or(here == 0, here == 3)

    def guarded(step, guard, make):
        @pl.when(guard)
        def _():
            make().start()

        def finish():
            @pl.when(guard)
            def _():
                make().wait_send()

        pending.setdefault(step, []).append(finish)

    def z_send_start(step, k, d, hop, guard):
        s = here - (hop - 1) if d == 0 else here + (hop - 1)
        target = here + 1 if d == 0 else here - 1
        guarded(step, guard, lambda: z_copy(k, d, hop, s, target, target))

    def own_send(step, k):
        for copy in chunks[k][1]:
            copy.wait()
        z_send_start(step, k, 0, 1, here <= 2)
        z_send_start(step, k, 1, 1, here >= 1)

    def extra_send(step, k):
        guarded(step, here <= 1, lambda: extra_copy(k, 0, here + 1))
        guarded(step, here >= 2, lambda: extra_copy(k, 1, here - 1))

    def arrive(step, k, d, hop):
        s = here - hop if d == 0 else here + hop
        origin = here - 1 if d == 0 else here + 1
        valid = here >= hop if d == 0 else here + hop <= 3

        @pl.when(valid)
        def _():
            z_copy(k, d, hop, s, origin, here).wait_recv()

        if hop < 3:
            onward = here <= 2 if d == 0 else here >= 1
            z_send_start(step, k, d, hop + 1, jnp.logical_and(valid, onward))
        crosses = jnp.logical_and(valid, at_end) if hop == 1 else valid
        cross = lambda: guarded(step, crosses, lambda: x_copy(k, d, hop, s, rep))
        if k == total - 1 and hop < 3:
            late.append(cross)
        else:
            cross()

    def x_arrive(k, d, hop):
        s = here - hop if d == 0 else here + hop
        valid = here >= hop if d == 0 else here + hop <= 3

        @pl.when(valid)
        def _():
            x_copy(k, d, hop, s, 1 - rep).wait_recv()

    def finish_sends(step):
        for finish in pending.pop(step, ()):
            finish()

    def sent_at(k):
        return max(0, k - 1)

    def advance(step, hop):
        if hop == 1:
            if step <= total:
                finish_sends(step - 2)
            for k in range(total):
                if sent_at(k) == step:
                    own_send(step, k)
                    if k == 0:
                        send_tokens()
            if step + first_copies < total:
                for copy in chunks[step + first_copies][1]:
                    copy.start()
        k = step - hop + 1
        if 0 <= k < total:
            for d in (0, 1):
                arrive(step, k, d, hop)
        if hop == 1 and 0 <= step - 1 < total:
            extra_send(step, step - 1)
        if hop == 3:
            while late:
                late.pop(0)()
        if hop == 3 and 0 <= step - 3 < total:
            for leg in (1, 2, 3):
                for d in (0, 1):
                    x_arrive(step - 3, d, leg)

    y_index = {}
    for name in ("gather1", "gather2", "reduce1"):
        for leg in ("beside", "across", "corner"):
            y_index[name, leg] = len(y_index) * seqs
    for leg in ("beside", "across", "corner"):
        y_index["reduce2", leg] = 9 * seqs + (len(y_index) - 9) * seqs * down_chunks

    send_group = {"gather1": 0, "gather2": 0, "reduce1": 1, "reduce2": 2}
    legs = ("beside", "across", "corner")

    def y_copy(name, leg, index, source, target, to, send_index=None):
        group = send_group[name] * 3 * seqs + legs.index(leg) * (2 * seqs if name == "reduce2" else seqs)
        return pltpu.make_async_remote_copy(
            src_ref=source, dst_ref=target,
            send_sem=y_send.at[group + (index if send_index is None else send_index)],
            recv_sem=y_recv.at[y_index[name, leg] + index], device_id={"tp": to}, device_id_type=MESH,
        )

    def seq_rows(j):
        return pl.ds(j * SEQ, SEQ)

    def gather_copy(name, buffer, leg, j, arriving):
        to = across_id if leg == "across" else beside_id
        source_of = {"beside": (tp, beside_id), "across": (tp, across_id), "corner": (across_id, corner_id)}
        owner = source_of[leg][1 if arriving else 0]
        view = buffer.at[seq_rows(j), own_rows(width, owner)]
        return y_copy(name, leg, j, view, view, to)

    y_pending = []

    def gather_send(name, buffer, leg, j):
        copy = gather_copy(name, buffer, leg, j, False)
        copy.start()
        y_pending.append(copy)

    def gather_wait(name, buffer, leg, j):
        gather_copy(name, buffer, leg, j, True).wait_recv()

    def relay(name, buffer, j):
        gather_wait(name, buffer, "across", j)
        gather_send(name, buffer, "corner", j)

    def norm_into(source, gain_ref, target, source_row, target_row):
        group = 16

        @pl.loop(0, SEQ // group, unroll=4)
        def _(i):
            offset = pl.multiple_of(i * group, group)
            floats = source[pl.ds(source_row + offset, group), :].astype(f32)
            scale = lax.rsqrt(jnp.mean(floats * floats, axis=-1, keepdims=True) + epsilon)
            target[pl.ds(target_row + offset, group), :] = (floats * scale * gain_ref[...]).astype(bf16)

    def make_mask():
        for copy in bring_small:
            copy.wait()
        gap = lax.broadcasted_iota(jnp.int32, (SEQ, SEQ), 0) - lax.broadcasted_iota(jnp.int32, (SEQ, SEQ), 1)
        positive = jnp.maximum(gap, 0).astype(f32)
        for head in range(heads):
            rate = rate_ref[pl.ds(tp * heads + head, 1), :]
            mask[head] = jnp.where(gap >= 0, jnp.exp(positive * rate), 0.0)

    def project(j):
        gather_wait("gather1", x_all, "beside", j)
        gather_wait("gather1", x_all, "corner", j)
        norm_into(x_all, mix_gain_ref, normed, j * SEQ, 0)
        proj[...] = jnp.dot(normed[...], w_mix[...], preferred_element_type=f32).astype(bf16)

    def retain():
        highest = lax.Precision.HIGHEST
        lane = lax.broadcasted_iota(jnp.int32, (SEQ, key_width), 1)
        cosine, sine = cos_ref[...], sin_ref[...]

        def turn(values):
            following = pltpu.roll(values, key_width - 1, 1)
            preceding = pltpu.roll(values, 1, 1)
            other = jnp.where(lane % 2 == 0, -following, preceding)
            return values * cosine + other * sine

        query = turn(proj[:, :key_width].astype(f32))
        key = turn(proj[:, key_width : 2 * key_width].astype(f32)) * DK ** (-0.5)
        for head in range(heads):
            only = jnp.where(lane // DK == head, query, 0.0)
            scores = lax.dot_general(
                only, key, (((1,), (1,)), ((), ())), precision=highest, preferred_element_type=f32
            ) * mask[head]
            first = 2 * key_width + head * DV
            value = proj[:, first : first + DV].astype(f32)
            retained = jnp.dot(scores, value, precision=highest, preferred_element_type=f32)
            centered = retained - jnp.mean(retained, axis=-1, keepdims=True)
            spread = jnp.mean(centered * centered, axis=-1, keepdims=True)
            grouped = centered * lax.rsqrt(spread + epsilon) * head_gain_ref[head : head + 1, :]
            first += value_width
            gate = proj[:, first : first + DV].astype(f32)
            mixed[:, head * DV : (head + 1) * DV] = (grouped * jax.nn.silu(gate)).astype(bf16)

    def reduce_copy(name, leg, index, source, target, send_index=None):
        to = across_id if leg == "across" else beside_id
        return y_copy(name, leg, index, source, target, to, send_index)

    def mix_reduce(j):
        def quarter(owner):
            return jnp.dot(mixed[...], w_out[:, own_rows(width, owner)], preferred_element_type=f32)

        def send(leg, source, target):
            copy = reduce_copy("reduce1", leg, j, source.at[j], target.at[j])
            copy.start()
            y_pending.append(copy)
            return copy

        corner1[j] = quarter(corner_id).astype(bf16)
        sent = send("corner", corner1, corner1_in)
        beside1[j] = quarter(beside_id).astype(bf16)
        send("beside", beside1, beside1_in)
        own1[j] = quarter(tp)
        far = quarter(across_id)
        sent.wait_recv()
        across1[j] = (far + corner1_in[j].astype(f32)).astype(bf16)
        send("across", across1, across1_in)

    def residual(j):
        reduce_copy("reduce1", "beside", j, beside1.at[j], beside1_in.at[j]).wait_recv()
        reduce_copy("reduce1", "across", j, across1.at[j], across1_in.at[j]).wait_recv()
        share = own1[j] + beside1_in[j].astype(f32) + across1_in[j].astype(f32)
        tokens = x_all[seq_rows(j), token_columns].astype(f32)
        res_all[seq_rows(j), token_columns] = (tokens + share).astype(bf16)
        gather_send("gather2", res_all, "across", j)
        gather_send("gather2", res_all, "beside", j)

    def ready(j):
        gather_wait("gather2", res_all, "beside", j)
        gather_wait("gather2", res_all, "corner", j)
        norm_into(res_all, ffn_gain_ref, normed_ffn, j * SEQ, j * SEQ)

    def ffn(b):
        group = FFN_ROWS * SEQ
        weight = w_ffn.at[:, pl.ds(b * pair_width, pair_width)]

        @pl.loop(0, rows // group)
        def _(j):
            part = own_rows(group, j)
            both = jnp.dot(normed_ffn[part, :], weight[...], preferred_element_type=f32)
            hidden[part, b * LANES : (b + 1) * LANES] = (
                jax.nn.silu(both[:, :LANES]) * both[:, LANES:]
            ).astype(bf16)

    def reduce2(leg, c, j, source, target):
        part = own_rows(SEQ, j)
        slot = (c % 2) * seqs + j
        return reduce_copy("reduce2", leg, c * seqs + j, source.at[c, part, :], target.at[c, part, :], slot)

    def down_products(c, j):
        part = own_rows(SEQ, j)
        if c + 1 < down_chunks:
            sums[...] = jnp.dot(hidden[part, :], w_down[c], preferred_element_type=f32)
        else:
            sums[...] = begun[part, :] + jnp.dot(
                hidden[part, split:], w_down[c, split:, :], preferred_element_type=f32
            )
        corner2[c, part, :] = sums[:, own_rows(LANES, corner_id)].astype(bf16)
        reduce2("corner", c, j, corner2, corner2_in).start()
        beside2[c, part, :] = sums[:, own_rows(LANES, beside_id)].astype(bf16)
        reduce2("beside", c, j, beside2, beside2_in).start()
        far2[part, :] = sums[:, own_rows(LANES, across_id)]
        own2[c, part, :] = sums[:, own_rows(LANES, tp)]

    def down_begin(c):
        @pl.loop(0, seqs)
        def _(j):
            part = own_rows(SEQ, j)
            begun[part, :] = jnp.dot(hidden[part, :split], w_down[c, :split, :], preferred_element_type=f32)

    def down_onward(c, j):
        part = own_rows(SEQ, j)
        reduce2("corner", c, j, corner2, corner2_in).wait_recv()
        across2[c, part, :] = (far2[part, :] + corner2_in[c, part, :].astype(f32)).astype(bf16)
        reduce2("across", c, j, across2, across2_in).start()

    def down(c):
        @pl.loop(0, seqs)
        def _(j):
            down_products(c, j)

    def down_rest(c):
        @pl.loop(0, seqs)
        def _(j):
            down_onward(c, j)

    def down_last(c):
        @pl.loop(0, seqs + 1)
        def _(j):
            @pl.when(j < seqs)
            def _():
                down_products(c, j)

            @pl.when(j > 0)
            def _():
                down_onward(c, j - 1)

    def finish_down(c):
        @pl.loop(0, seqs)
        def _(j):
            part = own_rows(SEQ, j)
            reduce2("beside", c, j, beside2, beside2_in).wait_recv()
            reduce2("across", c, j, across2, across2_in).wait_recv()
            share = own2[c, part, :] + beside2_in[c, part, :].astype(f32) + across2_in[c, part, :].astype(f32)
            columns = pl.ds(pl.multiple_of(tp * width + c * LANES, LANES), LANES)
            kept = res_all[part, columns].astype(f32)
            result[c, part, :] = (kept + share).astype(bf16)
            for leg, source, target in (
                ("corner", corner2, corner2_in), ("beside", beside2, beside2_in), ("across", across2, across2_in),
            ):
                reduce2(leg, c, j, source, target).wait_send()

        out_copy(c).start()

    def out_copy(c):
        return pltpu.make_async_copy(result.at[c], out_ref.at[:, pl.ds(c * LANES, LANES)], out_sem.at[c])

    work = {}

    def at(slot, function, *args):
        work.setdefault(slot, []).append((function, args))

    at(0, make_mask)
    for j in range(seqs):
        at(5 + 3 * j, relay, "gather1", x_all, j)
    base = 3 * (mix_chunks + 2) + 2
    for j, (a, b, r, s, l, n) in enumerate(PLAN):
        at(base + s, residual, j)
        at(base + l, relay, "gather2", res_all, j)
        at(base + n, ready, j)
        at(base + b, retain)
        at(base + r, mix_reduce, j)
        at(base + a, project, j)
    def finish_gather():
        for copy in y_pending[: 3 * seqs]:
            copy.wait_send()
        del y_pending[: 3 * seqs]

    at(base + min(r for _, _, r, *_ in PLAN), finish_gather)
    slot = base + 1 + max(n for *_, n in PLAN)
    for block in range(ffn_blocks):
        slot = max(slot, 3 * (first_ffn + block + 3) + 2)
        at(slot, ffn, block)
        slot += 1 if slot % 3 != FFN_PER_STEP - 1 else 4 - FFN_PER_STEP
    for c in range(down_chunks - 1):
        complete = 3 * (first_down + 3 + c) + 2
        if c + 2 < down_chunks:
            at(complete, down, c)
            at(complete + 1, down_rest, c)
        else:
            at(complete, down_last, c)
        if c + 2 < down_chunks:
            at(complete + 5, finish_down, c)
    last_slot = 3 * (total + 3) - 1
    at(last_slot - 3, down_begin, down_chunks - 1)

    def send_tokens():
        bring_tokens.wait()
        for j in range(seqs):
            gather_send("gather1", x_all, "across", j)
            gather_send("gather1", x_all, "beside", j)

    for slot in range(3 * (total + 3)):
        advance(slot // 3, slot % 3 + 1)
        for function, args in work.get(slot, ()):
            function(*args)
    down_last(down_chunks - 1)
    finish_down(down_chunks - 2)
    finish_down(down_chunks - 1)
    for step in sorted(pending):
        finish_sends(step)
    for copy in y_pending:
        copy.wait_send()
    for c in range(down_chunks):
        out_copy(c).wait()


def layer(
    tokens, mix_gain, query_weight, key_weight, value_weight, gate_weight, out_weight, head_gain,
    ffn_gain, ffn_gate, ffn_up, ffn_down,
):
    bf16, f32 = jnp.bfloat16, jnp.float32
    rows, width = tokens.shape
    model = 4 * width
    seqs = rows // SEQ
    key_width, value_width = query_weight.shape[1], value_weight.shape[1]
    heads = head_gain.shape[0]
    mix_width = 2 * key_width + 2 * value_width
    hidden_width = ffn_gate.shape[1]
    blocks, down_chunks = hidden_width // LANES, ffn_down.shape[1] // LANES
    total = mix_width // (2 * LANES) + 1 + blocks + down_chunks + 1
    frequency = rope_base ** (-np.linspace(0.0, 1.0, DK // 2))
    angles = np.arange(SEQ)[:, None] * frequency[None, :]
    cosine = np.tile(np.repeat(np.cos(angles), 2, axis=1), (1, heads)).astype(np.float32)
    sine = np.tile(np.repeat(np.sin(angles), 2, axis=1), (1, heads)).astype(np.float32)
    rates = np.log1p(-np.exp2(-5.0 - 4.0 * np.arange(HEADS) / (HEADS - 1)))
    rates = np.broadcast_to(rates[:, None], (HEADS, SEQ)).astype(np.float32)
    anywhere = pl.BlockSpec(memory_space=pl.ANY)
    first_sum = [pltpu.VMEM((seqs, SEQ, width), bf16)] * 6
    second_sum = [pltpu.VMEM((down_chunks, rows, LANES), bf16)] * 6
    dma = pltpu.SemaphoreType.DMA
    return pl.pallas_call(
        fused_kernel,
        out_shape=jax.ShapeDtypeStruct((rows, width), bf16),
        in_specs=[anywhere] * 15,
        out_specs=anywhere,
        scratch_shapes=[
            pltpu.VMEM((1, model), f32),
            pltpu.VMEM(head_gain.shape, f32),
            pltpu.VMEM((1, model), f32),
            pltpu.VMEM(cosine.shape, f32),
            pltpu.VMEM(sine.shape, f32),
            pltpu.VMEM(rates.shape, f32),
            pltpu.VMEM((model, mix_width), bf16),
            pltpu.VMEM((out_weight.shape[0], model), bf16),
            pltpu.VMEM((model, 2 * hidden_width), bf16),
            pltpu.VMEM((down_chunks, hidden_width, 4 * LANES), bf16),
            pltpu.VMEM((rows, model), bf16),
            pltpu.VMEM((rows, model), bf16),
            pltpu.VMEM((SEQ, model), bf16),
            pltpu.VMEM((rows, model), bf16),
            pltpu.VMEM((SEQ, mix_width), bf16),
            pltpu.VMEM((SEQ, heads * DV), bf16),
            pltpu.VMEM((rows, hidden_width), bf16),
            pltpu.VMEM((heads, SEQ, SEQ), f32),
        ]
        + first_sum
        + [pltpu.VMEM((seqs, SEQ, width), f32)]
        + second_sum
        + [
            pltpu.VMEM((down_chunks, rows, LANES), f32),
            pltpu.VMEM((rows, LANES), f32),
            pltpu.VMEM((SEQ, 4 * LANES), f32),
            pltpu.VMEM((rows, 4 * LANES), f32),
            pltpu.VMEM((down_chunks, rows, LANES), bf16),
        ]
        + [
            dma((20 + down_chunks,)),
            dma((3, 2, 4)),
            dma((total, 3)),
            dma((3, 2, 3)),
            dma((total, 3)),
            dma((12 * seqs,)),
            dma((9 * seqs + 3 * seqs * down_chunks,)),
            dma((down_chunks,)),
        ],
        compiler_params=pltpu.CompilerParams(
            collective_id=0, has_side_effects=True, vmem_limit_bytes=67043328
        ),
        name="layer",
    )(
        tokens, mix_gain.reshape(1, -1), query_weight, key_weight, value_weight, gate_weight, out_weight,
        head_gain, ffn_gain.reshape(1, -1), ffn_gate, ffn_up, ffn_down, cosine, sine, rates,
    )


def solution(mesh):
    shape = mesh.shape
    small = shape["rep"] == 2 and shape["fs"] == 4 and shape["tp"] == 4
    return jax.shard_map(
        layer if small else per_device_plain,
        mesh=mesh,
        in_specs=(
            P(("rep", "fs"), "tp"),
            P(),
            P("fs", "tp"),
            P("fs", "tp"),
            P("fs", "tp"),
            P("fs", "tp"),
            P("tp", "fs"),
            P("tp", None),
            P(),
            P("fs", "tp"),
            P("fs", "tp"),
            P("tp", "fs"),
        ),
        out_specs=P(("rep", "fs"), "tp"),
        check_vma=False,
    )
```

```python
import jax
import jax.numpy as jnp
import numpy as np
from jax import lax
from jax.experimental import pallas as pl
from jax.experimental.pallas import tpu as pltpu
from jax.sharding import PartitionSpec as P

HEADS = 8
DK = 64
DV = 128
BLOCK = 64
SEQ = 256


epsilon = 1e-06
rope_base = 10000.0


def norm_rows(values, gain_row):
    floats = values.astype(jnp.float32)
    scaled = floats * lax.rsqrt(jnp.mean(floats * floats, axis=-1, keepdims=True) + epsilon)
    return (scaled * gain_row).astype(jnp.bfloat16)


def rotate(values, positions):
    half_dim = values.shape[-1] // 2
    frequency = rope_base ** (-jnp.linspace(0.0, 1.0, half_dim, dtype=jnp.float32))
    angles = positions.astype(jnp.float32)[:, None] * frequency[None, :]
    cosine = jnp.cos(angles)[:, None, :]
    sine_part = jnp.sin(angles)[:, None, :]
    paired = values.reshape(values.shape[:-1] + (half_dim, 2))
    leading = paired[..., 0]
    trailing = paired[..., 1]
    turned = jnp.stack(
        [leading * cosine - trailing * sine_part, leading * sine_part + trailing * cosine], axis=-1
    )
    return turned.reshape(values.shape)


def log_decay(head_index, total_heads):
    return jnp.log1p(-jnp.exp2(-5.0 - 4.0 * head_index.astype(jnp.float32) / (total_heads - 1)))


def retention(queries, key_rows, value_rows, decay_rates):
    highest = lax.Precision.HIGHEST
    row_count, head_count = (queries.shape[0], queries.shape[1])
    seq_count = row_count // SEQ
    block_count = SEQ // BLOCK

    def to_blocks(values):
        shaped = values.reshape((seq_count, block_count, BLOCK) + values.shape[1:])
        return jnp.moveaxis(shaped, 1, 0)

    inside = jnp.arange(BLOCK, dtype=jnp.int32)
    gap = (inside[:, None] - inside[None, :]).astype(jnp.float32)
    within_mask = jnp.where(
        gap[None] >= 0.0, jnp.exp(jnp.maximum(gap, 0.0)[None] * decay_rates[:, None, None]), 0.0
    )
    query_scale = jnp.exp((inside + 1).astype(jnp.float32)[:, None] * decay_rates[None, :])
    key_scale = jnp.exp((BLOCK - 1 - inside).astype(jnp.float32)[:, None] * decay_rates[None, :])
    block_decay = jnp.exp(BLOCK * decay_rates)

    def advance(state, inputs):
        query_blk, key_blk, value_blk = inputs
        scores = (
            jnp.einsum("sihd,sjhd->shij", query_blk, key_blk, precision=highest) * within_mask[None]
        )
        local_part = jnp.einsum("shij,sjhv->sihv", scores, value_blk, precision=highest)
        carried = jnp.einsum(
            "sihd,shdv->sihv", query_blk * query_scale[None, :, :, None], state, precision=highest
        )
        update = jnp.einsum(
            "sjhd,sjhv->shdv", key_blk * key_scale[None, :, :, None], value_blk, precision=highest
        )
        return (block_decay[None, :, None, None] * state + update, local_part + carried)

    state_zero = jnp.zeros((seq_count, head_count, DK, DV), jnp.float32)
    _, outputs = lax.scan(
        advance, state_zero, (to_blocks(queries), to_blocks(key_rows), to_blocks(value_rows))
    )
    return jnp.moveaxis(outputs, 0, 1).reshape(row_count, head_count, DV)


def per_device_plain(
    tokens,
    mix_gain,
    query_weight,
    key_weight,
    value_weight,
    gate_weight,
    out_weight,
    head_gain,
    ffn_gain,
    ffn_gate,
    ffn_up,
    ffn_down,
):
    whole_rows = lax.all_gather(tokens, "tp", axis=1, tiled=True)
    row_count = whole_rows.shape[0]
    normed = norm_rows(whole_rows, mix_gain)
    pieces = (
        lax.all_gather(query_weight, "fs", axis=0, tiled=True),
        lax.all_gather(key_weight, "fs", axis=0, tiled=True),
        lax.all_gather(value_weight, "fs", axis=0, tiled=True),
        lax.all_gather(gate_weight, "fs", axis=0, tiled=True),
    )
    query_acc, key_acc, value_acc, gate_acc = tuple(
        (
            jnp.dot(normed, weight_piece, preferred_element_type=jnp.float32)
            for weight_piece in pieces
        )
    )
    heads_here = query_weight.shape[1] // DK
    positions = jnp.arange(row_count, dtype=jnp.int32) % SEQ
    queries = rotate(
        query_acc.astype(jnp.bfloat16).astype(jnp.float32).reshape(row_count, heads_here, DK),
        positions,
    )
    key_rows = rotate(
        key_acc.astype(jnp.bfloat16).astype(jnp.float32).reshape(row_count, heads_here, DK),
        positions,
    ) * DK ** (-0.5)
    value_rows = (
        value_acc.astype(jnp.bfloat16).astype(jnp.float32).reshape(row_count, heads_here, DV)
    )
    gate_rows = gate_acc.astype(jnp.bfloat16).astype(jnp.float32)
    first_head = lax.axis_index("tp") * heads_here
    decay_rates = log_decay(first_head + jnp.arange(heads_here, dtype=jnp.int32), HEADS)
    retained = retention(queries, key_rows, value_rows, decay_rates)
    center = jnp.mean(retained, axis=-1, keepdims=True)
    spread = jnp.mean(jnp.square(retained - center), axis=-1, keepdims=True)
    grouped = (retained - center) * lax.rsqrt(spread + epsilon) * head_gain[None]
    mixed = (grouped.reshape(row_count, heads_here * DV) * jax.nn.silu(gate_rows)).astype(
        jnp.bfloat16
    )
    mixer_terms = jnp.dot(
        mixed,
        lax.all_gather(out_weight, "fs", axis=1, tiled=True),
        preferred_element_type=jnp.float32,
    )
    mixer_share = lax.psum_scatter(
        mixer_terms.astype(jnp.bfloat16), "tp", scatter_dimension=1, tiled=True
    ).astype(jnp.float32)
    resid_shard = (tokens.astype(jnp.float32) + mixer_share).astype(jnp.bfloat16)
    resid_whole = lax.all_gather(resid_shard, "tp", axis=1, tiled=True)
    normed_ffn = norm_rows(resid_whole, ffn_gain)

    def add_rows(weight_piece):
        return jnp.dot(normed_ffn, weight_piece, preferred_element_type=jnp.float32)

    gate_hidden = add_rows(lax.all_gather(ffn_gate, "fs", axis=0, tiled=True))
    up_hidden = add_rows(lax.all_gather(ffn_up, "fs", axis=0, tiled=True))
    hidden = (jax.nn.silu(gate_hidden) * up_hidden).astype(jnp.bfloat16)
    ffn_terms = jnp.dot(
        hidden,
        lax.all_gather(ffn_down, "fs", axis=1, tiled=True),
        preferred_element_type=jnp.float32,
    )
    ffn_share = lax.psum_scatter(
        ffn_terms.astype(jnp.bfloat16), "tp", scatter_dimension=1, tiled=True
    ).astype(jnp.float32)
    return (resid_shard.astype(jnp.float32) + ffn_share).astype(jnp.bfloat16)


MESH = pl.DeviceIdType.MESH
LANES = 128
FFN_ROWS = 2
FFN_BLOCKS = 1
FFN_STRIDE = 1
PLAN = ((0, 1, 3, 6, 10, 12), (2, 4, 5, 8, 14, 16), (5, 6, 7, 12, 19, 20), (8, 9, 11, 17, 21, 22))


def fused_kernel(
    tokens_ref, mix_gain_hbm, query_ref, key_ref, value_ref, gate_ref, proj_out_ref, head_gain_hbm,
    ffn_gain_hbm, ffn_gate_ref, ffn_up_ref, ffn_down_ref, cos_hbm, sin_hbm, rate_hbm,
    out_ref,
    mix_gain_ref, head_gain_ref, ffn_gain_ref, cos_ref, sin_ref, rate_ref,
    w_mix, w_out, w_ffn, w_down, x_all, res_all, normed, normed_ffn, proj, mixed, hidden, mask,
    corner1, corner1_in, beside1, beside1_in, across1, across1_in, own1,
    corner2, corner2_in, beside2, beside2_in, across2, across2_in, own2, far2, sums, result,
    local_sem, z_send, z_recv, x_send, x_recv, y_send, y_recv, out_sem,
):
    f32, bf16 = jnp.float32, jnp.bfloat16
    rep, here, tp = lax.axis_index("rep"), lax.axis_index("fs"), lax.axis_index("tp")
    core, chip = tp % 2, tp // 2
    beside_id, across_id, corner_id = tp + 1 - 2 * core, (tp + 2) % 4, 3 - tp
    rows, width = tokens_ref.shape
    seqs = rows // SEQ
    shard = query_ref.shape[0]
    key_width, value_width = query_ref.shape[1], value_ref.shape[1]
    heads = head_gain_ref.shape[0]
    ffn_blocks = ffn_gate_ref.shape[1] // LANES
    down_chunks = ffn_down_ref.shape[1] // LANES
    pair_width = 2 * LANES

    def own_rows(size, base=None):
        index = here if base is None else base
        return pl.ds(pl.multiple_of(index * size, size), size)

    barrier = pltpu.get_barrier_semaphore()
    for target in (
        {"fs": (here + 1) % 4}, {"fs": (here + 3) % 4}, {"rep": 1 - rep}, {"tp": beside_id}, {"tp": across_id},
    ):
        pl.semaphore_signal(barrier, inc=1, device_id=target, device_id_type=MESH)

    def bring(slot, source, target):
        return pltpu.make_async_copy(source, target, local_sem.at[slot])

    token_columns = own_rows(width, tp)
    bring_tokens = bring(0, tokens_ref, x_all.at[:, token_columns])
    bring_mix = []
    start = 0
    for ref in (query_ref, key_ref, value_ref, gate_ref):
        bring_mix.append(bring(1 + len(bring_mix), ref, w_mix.at[own_rows(shard), pl.ds(start, ref.shape[1])]))
        start += ref.shape[1]
    bring_out = bring(5, proj_out_ref, w_out.at[:, own_rows(proj_out_ref.shape[1])])
    bring_ffn = [
        [
            bring(
                6 + 2 * (block % 4) + part,
                ref.at[:, pl.ds(block * LANES, LANES)],
                w_ffn.at[own_rows(shard), pl.ds(block * pair_width + part * LANES, LANES)],
            )
            for part, ref in enumerate((ffn_gate_ref, ffn_up_ref))
        ]
        for block in range(ffn_blocks)
    ]
    bring_down = [
        bring(14 + c, ffn_down_ref.at[:, pl.ds(c * LANES, LANES)], w_down.at[c, :, own_rows(LANES)])
        for c in range(down_chunks)
    ]

    chunks = []
    mix_chunks = w_mix.shape[1] // pair_width
    half_shard = shard // 2

    def row_chunk(buffer, column):
        def view(s, half):
            first = pl.multiple_of(s * shard + half * half_shard, half_shard)
            return buffer.at[pl.ds(first, half_shard), pl.ds(column, pair_width)]

        return view

    for i in range(mix_chunks):
        needs = {0: bring_mix[:2], 1: bring_mix[2:3], 2: bring_mix[3:]}[i]
        chunks.append((row_chunk(w_mix, i * pair_width), needs))

    def out_view(s, half):
        size, columns = w_out.shape[0] // 2, proj_out_ref.shape[1]
        return w_out.at[own_rows(size, half), own_rows(columns, s)]

    chunks.append((out_view, [bring_out]))
    for block in range(ffn_blocks):
        chunks.append((row_chunk(w_ffn, block * pair_width), bring_ffn[block]))

    def down_view(c):
        def view(s, half):
            return w_down.at[c, own_rows(w_down.shape[1] // 2, half), own_rows(LANES, s)]

        return view

    for c in range(down_chunks):
        chunks.append((down_view(c), [bring_down[c]]))
    chunks.append((down_view(down_chunks - 1), []))
    total = len(chunks)

    def travels(k, s):
        if k < total - 2:
            return True
        other_chip = jnp.logical_xor(s >= 2, chip == 1)
        return other_chip if k == total - 2 else jnp.logical_not(other_chip)

    def allowed(guard, k, s):
        return guard if k < total - 2 else jnp.logical_and(guard, travels(k, s))

    first_ffn = mix_chunks + 1
    first_down = first_ffn + ffn_blocks
    first_copies = 5

    for k in range(first_copies):
        if k == 1:
            bring_tokens.start()
        for copy in chunks[k][1]:
            copy.start()
    bring_small = [
        bring(14 + down_chunks + i, source, target)
        for i, (source, target) in enumerate(
            (
                (mix_gain_hbm, mix_gain_ref), (head_gain_hbm, head_gain_ref), (ffn_gain_hbm, ffn_gain_ref),
                (cos_hbm, cos_ref), (sin_hbm, sin_ref), (rate_hbm, rate_ref),
            )
        )
    ]
    for copy in bring_small:
        copy.start()
    pl.semaphore_wait(barrier, 5)

    def place(d, hop, receiver):
        return hop - 1 if d == 0 else receiver + hop - 1

    def z_copy(k, d, hop, s, target, receiver):
        view = chunks[k][0](s, rep)
        return pltpu.make_async_remote_copy(
            src_ref=view, dst_ref=view, send_sem=z_send.at[k % 3, d, hop - 1],
            recv_sem=z_recv.at[k, place(d, hop, receiver)], device_id={"fs": target}, device_id_type=MESH,
        )

    def extra_copy(k, d, target):
        view = chunks[k][0](here, 1 - rep)
        return pltpu.make_async_remote_copy(
            src_ref=view, dst_ref=view, send_sem=z_send.at[k % 3, d, 3],
            recv_sem=x_recv.at[k, place(d, 1, target)], device_id={"fs": target}, device_id_type=MESH,
        )

    def x_copy(k, d, hop, s, half):
        view = chunks[k][0](s, half)
        return pltpu.make_async_remote_copy(
            src_ref=view, dst_ref=view, send_sem=x_send.at[k % 3, d, hop - 1],
            recv_sem=x_recv.at[k, place(d, hop, here)], device_id={"rep": 1 - rep}, device_id_type=MESH,
        )

    pending = {}
    late = []

    def guarded(step, guard, make):
        @pl.when(guard)
        def _():
            make().start()

        def finish():
            @pl.when(guard)
            def _():
                make().wait_send()

        pending.setdefault(step, []).append(finish)

    def z_send_start(step, k, d, hop, guard):
        s = here - (hop - 1) if d == 0 else here + (hop - 1)
        target = here + 1 if d == 0 else here - 1
        guarded(step, allowed(guard, k, s), lambda: z_copy(k, d, hop, s, target, target))

    def own_send(step, k):
        for copy in chunks[k][1]:
            copy.wait()
        z_send_start(step, k, 0, 1, here <= 2)
        z_send_start(step, k, 1, 1, here >= 1)

    def extra_send(step, k):
        guarded(step, allowed(here == 0, k, here), lambda: extra_copy(k, 0, here + 1))
        guarded(step, allowed(here == 3, k, here), lambda: extra_copy(k, 1, here - 1))

    def arrive(step, k, d, hop):
        s = here - hop if d == 0 else here + hop
        origin = here - 1 if d == 0 else here + 1
        valid = allowed(here >= hop if d == 0 else here + hop <= 3, k, s)

        @pl.when(valid)
        def _():
            z_copy(k, d, hop, s, origin, here).wait_recv()

        if hop < 3:
            onward = here <= 2 if d == 0 else here >= 1
            z_send_start(step, k, d, hop + 1, jnp.logical_and(valid, onward))
        crosses = jnp.logical_and(valid, here != 1 + d) if hop == 1 else valid
        cross = lambda: guarded(step, crosses, lambda: x_copy(k, d, hop, s, rep))
        if k == total - 1 and hop < 3:
            late.append(cross)
        else:
            cross()

    def x_arrive(k, d, hop):
        s = here - hop if d == 0 else here + hop
        valid = allowed(here >= hop if d == 0 else here + hop <= 3, k, s)

        @pl.when(valid)
        def _():
            x_copy(k, d, hop, s, 1 - rep).wait_recv()

    def finish_sends(step):
        for finish in pending.pop(step, ()):
            finish()

    def complete_at(k):
        return 3 * (k + 3) + 2

    def sent_at(k):
        return max(0, k - 1)

    def advance(step, hop):
        if hop == 1:
            if step <= total:
                finish_sends(step - 2)
            for k in range(total):
                if sent_at(k) == step:
                    own_send(step, k)
                    if k == 0:
                        send_tokens()
            if step + first_copies < total:
                for copy in chunks[step + first_copies][1]:
                    copy.start()
        k = step - hop + 1
        if 0 <= k < total:
            for d in (0, 1):
                arrive(step, k, d, hop)
        if hop == 1 and 0 <= step - 1 < total:
            extra_send(step, step - 1)
        if hop == 3:
            while late and step >= total:
                late.pop(0)()
        for k in range(total):
            if complete_at(k) == 3 * step + hop - 1:
                for leg in (1, 2, 3):
                    for d in (0, 1):
                        x_arrive(k, d, leg)

    y_index = {}
    for name in ("gather1", "gather2", "reduce1"):
        for leg in ("beside", "across", "corner"):
            y_index[name, leg] = len(y_index) * seqs
    for leg in ("beside", "across", "corner"):
        y_index["reduce2", leg] = 9 * seqs + (len(y_index) - 9) * seqs * down_chunks

    send_group = {"gather1": 0, "gather2": 0, "reduce1": 1, "reduce2": 2}
    legs = ("beside", "across", "corner")

    def y_copy(name, leg, index, source, target, to, send_index=None):
        group = send_group[name] * 3 * seqs + legs.index(leg) * (3 * seqs if name == "reduce2" else seqs)
        return pltpu.make_async_remote_copy(
            src_ref=source, dst_ref=target,
            send_sem=y_send.at[group + (index if send_index is None else send_index)],
            recv_sem=y_recv.at[y_index[name, leg] + index], device_id={"tp": to}, device_id_type=MESH,
        )

    def seq_rows(j):
        return pl.ds(j * SEQ, SEQ)

    def gather_copy(name, buffer, leg, j, arriving):
        to = across_id if leg == "across" else beside_id
        source_of = {"beside": (tp, beside_id), "across": (tp, across_id), "corner": (across_id, corner_id)}
        owner = source_of[leg][1 if arriving else 0]
        view = buffer.at[seq_rows(j), own_rows(width, owner)]
        return y_copy(name, leg, j, view, view, to)

    y_pending = []

    def gather_send(name, buffer, leg, j):
        copy = gather_copy(name, buffer, leg, j, False)
        copy.start()
        y_pending.append(copy)

    def gather_wait(name, buffer, leg, j):
        gather_copy(name, buffer, leg, j, True).wait_recv()

    def relay(name, buffer, j):
        gather_wait(name, buffer, "across", j)
        gather_send(name, buffer, "corner", j)

    def norm_into(source, gain_ref, target, source_row, target_row):
        group = 16

        @pl.loop(0, SEQ // group, unroll=4)
        def _(i):
            offset = pl.multiple_of(i * group, group)
            floats = source[pl.ds(source_row + offset, group), :].astype(f32)
            scale = lax.rsqrt(jnp.mean(floats * floats, axis=-1, keepdims=True) + epsilon)
            target[pl.ds(target_row + offset, group), :] = (floats * scale * gain_ref[...]).astype(bf16)

    def make_mask():
        for copy in bring_small:
            copy.wait()
        gap = lax.broadcasted_iota(jnp.int32, (SEQ, SEQ), 0) - lax.broadcasted_iota(jnp.int32, (SEQ, SEQ), 1)
        positive = jnp.maximum(gap, 0).astype(f32)
        for head in range(heads):
            rate = rate_ref[pl.ds(tp * heads + head, 1), :]
            mask[head] = jnp.where(gap >= 0, jnp.exp(positive * rate), 0.0)

    def project(j):
        gather_wait("gather1", x_all, "beside", j)
        gather_wait("gather1", x_all, "corner", j)
        norm_into(x_all, mix_gain_ref, normed, j * SEQ, 0)
        proj[...] = jnp.dot(normed[...], w_mix[...], preferred_element_type=f32).astype(bf16)

    def retain():
        highest = lax.Precision.HIGHEST
        lane = lax.broadcasted_iota(jnp.int32, (SEQ, key_width), 1)
        cosine, sine = cos_ref[...], sin_ref[...]

        def turn(values):
            following = pltpu.roll(values, key_width - 1, 1)
            preceding = pltpu.roll(values, 1, 1)
            other = jnp.where(lane % 2 == 0, -following, preceding)
            return values * cosine + other * sine

        query = turn(proj[:, :key_width].astype(f32))
        key = turn(proj[:, key_width : 2 * key_width].astype(f32)) * DK ** (-0.5)
        for head in range(heads):
            only = jnp.where(lane // DK == head, query, 0.0)
            scores = lax.dot_general(
                only, key, (((1,), (1,)), ((), ())), precision=highest, preferred_element_type=f32
            ) * mask[head]
            first = 2 * key_width + head * DV
            value = proj[:, first : first + DV].astype(f32)
            retained = jnp.dot(scores, value, precision=highest, preferred_element_type=f32)
            centered = retained - jnp.mean(retained, axis=-1, keepdims=True)
            spread = jnp.mean(centered * centered, axis=-1, keepdims=True)
            grouped = centered * lax.rsqrt(spread + epsilon) * head_gain_ref[head : head + 1, :]
            first += value_width
            gate = proj[:, first : first + DV].astype(f32)
            mixed[:, head * DV : (head + 1) * DV] = (grouped * jax.nn.silu(gate)).astype(bf16)

    def reduce_copy(name, leg, index, source, target, send_index=None):
        to = across_id if leg == "across" else beside_id
        return y_copy(name, leg, index, source, target, to, send_index)

    def mix_reduce(j):
        def quarter(owner):
            return jnp.dot(mixed[...], w_out[:, own_rows(width, owner)], preferred_element_type=f32)

        def send(leg, source, target):
            copy = reduce_copy("reduce1", leg, j, source.at[j], target.at[j])
            copy.start()
            y_pending.append(copy)
            return copy

        corner1[j] = quarter(corner_id).astype(bf16)
        sent = send("corner", corner1, corner1_in)
        beside1[j] = quarter(beside_id).astype(bf16)
        send("beside", beside1, beside1_in)
        own1[j] = quarter(tp)
        far = quarter(across_id)
        sent.wait_recv()
        across1[j] = (far + corner1_in[j].astype(f32)).astype(bf16)
        send("across", across1, across1_in)

    def residual(j):
        reduce_copy("reduce1", "beside", j, beside1.at[j], beside1_in.at[j]).wait_recv()
        reduce_copy("reduce1", "across", j, across1.at[j], across1_in.at[j]).wait_recv()
        share = own1[j] + beside1_in[j].astype(f32) + across1_in[j].astype(f32)
        tokens = x_all[seq_rows(j), token_columns].astype(f32)
        res_all[seq_rows(j), token_columns] = (tokens + share).astype(bf16)
        gather_send("gather2", res_all, "across", j)
        gather_send("gather2", res_all, "beside", j)

    def ready(j):
        gather_wait("gather2", res_all, "beside", j)
        gather_wait("gather2", res_all, "corner", j)
        norm_into(res_all, ffn_gain_ref, normed_ffn, j * SEQ, j * SEQ)

    def ffn(b, count):
        group = FFN_ROWS * SEQ
        weight = w_ffn.at[:, pl.ds(b * pair_width, count * pair_width)]

        @pl.loop(0, rows // group)
        def _(j):
            part = own_rows(group, j)
            both = jnp.dot(normed_ffn[part, :], weight[...], preferred_element_type=f32)
            for i in range(count):
                first = i * pair_width
                hidden[part, (b + i) * LANES : (b + i + 1) * LANES] = (
                    jax.nn.silu(both[:, first : first + LANES]) * both[:, first + LANES : first + pair_width]
                ).astype(bf16)

    def reduce2(leg, c, j, source, target):
        part = own_rows(SEQ, j)
        slot = (c % 2 if c + 1 < down_chunks else 2) * seqs + j
        return reduce_copy("reduce2", leg, c * seqs + j, source.at[c, part, :], target.at[c, part, :], slot)

    def keep_far(c, j, corner, across):
        part = own_rows(SEQ, j)
        corner2[c, part, :] = corner.astype(bf16)
        reduce2("corner", c, j, corner2, corner2_in).start()
        far2[part, :] = across

    def keep_near(c, j, beside, own):
        part = own_rows(SEQ, j)
        beside2[c, part, :] = beside.astype(bf16)
        reduce2("beside", c, j, beside2, beside2_in).start()
        own2[c, part, :] = own

    def down_products(c, j):
        sums[...] = jnp.dot(hidden[own_rows(SEQ, j), :], w_down[c], preferred_element_type=f32)
        keep_far(c, j, sums[:, own_rows(LANES, corner_id)], sums[:, own_rows(LANES, across_id)])
        keep_near(c, j, sums[:, own_rows(LANES, beside_id)], sums[:, own_rows(LANES, tp)])

    def pair_products(c, j, which):
        weight = w_down[c, :, own_rows(pair_width, which)]
        sums[:, :pair_width] = jnp.dot(hidden[own_rows(SEQ, j), :], weight, preferred_element_type=f32)
        return sums[:, own_rows(LANES, 1 - core)], sums[:, own_rows(LANES, core)]

    def far_products(c, j):
        keep_far(c, j, *pair_products(c, j, 1 - chip))

    def down_near(c):
        @pl.loop(0, seqs)
        def _(j):
            keep_near(c, j, *pair_products(c, j, chip))

    def down_onward(c, j):
        part = own_rows(SEQ, j)
        reduce2("corner", c, j, corner2, corner2_in).wait_recv()
        across2[c, part, :] = (far2[part, :] + corner2_in[c, part, :].astype(f32)).astype(bf16)
        reduce2("across", c, j, across2, across2_in).start()

    def down(c):
        @pl.loop(0, seqs)
        def _(j):
            down_products(c, j)

    def down_rest(c):
        @pl.loop(0, seqs)
        def _(j):
            down_onward(c, j)

    def down_piped(c, products):
        @pl.loop(0, seqs + 1)
        def _(j):
            @pl.when(j < seqs)
            def _():
                products(c, j)

            @pl.when(j > 0)
            def _():
                down_onward(c, j - 1)

    def finish_down(c):
        @pl.loop(0, seqs)
        def _(j):
            part = own_rows(SEQ, j)
            reduce2("beside", c, j, beside2, beside2_in).wait_recv()
            reduce2("across", c, j, across2, across2_in).wait_recv()
            share = own2[c, part, :] + beside2_in[c, part, :].astype(f32) + across2_in[c, part, :].astype(f32)
            columns = pl.ds(pl.multiple_of(tp * width + c * LANES, LANES), LANES)
            kept = res_all[part, columns].astype(f32)
            result[c, part, :] = (kept + share).astype(bf16)
            for leg, source, target in (
                ("corner", corner2, corner2_in), ("beside", beside2, beside2_in), ("across", across2, across2_in),
            ):
                reduce2(leg, c, j, source, target).wait_send()

        out_copy(c).start()

    def out_copy(c):
        return pltpu.make_async_copy(result.at[c], out_ref.at[:, pl.ds(c * LANES, LANES)], out_sem.at[c])

    work = {}

    def at(slot, function, *args):
        work.setdefault(slot, []).append((function, args))

    at(0, make_mask)
    for j in range(seqs):
        at(5 + 3 * j, relay, "gather1", x_all, j)
    base = 3 * (mix_chunks + 2) + 2
    for j, (a, b, r, s, l, n) in enumerate(PLAN):
        at(base + s, residual, j)
        at(base + l, relay, "gather2", res_all, j)
        at(base + n, ready, j)
        at(base + b, retain)
        at(base + r, mix_reduce, j)
        at(base + a, project, j)
    def finish_gather():
        for copy in y_pending[: 3 * seqs]:
            copy.wait_send()
        del y_pending[: 3 * seqs]

    at(base + min(r for _, _, r, *_ in PLAN), finish_gather)
    slot = base + 1 + max(n for *_, n in PLAN)
    for block in range(0, ffn_blocks, FFN_BLOCKS):
        count = min(FFN_BLOCKS, ffn_blocks - block)
        slot = max(slot, 3 * (first_ffn + block + count - 1 + 3) + 2)
        at(slot, ffn, block, count)
        slot += FFN_STRIDE
    for c in range(down_chunks - 1):
        complete = complete_at(first_down + c)
        if c + 2 < down_chunks:
            at(complete, down, c)
            at(complete + 1, down_rest, c)
            if c + 3 < down_chunks:
                at(3 * (first_down + c + 5), finish_down, c)
        else:
            at(complete, down_piped, c, down_products)
    last = down_chunks - 1
    at(complete_at(total - 2), down_piped, last, far_products)

    def send_tokens():
        bring_tokens.wait()
        for j in range(seqs):
            gather_send("gather1", x_all, "across", j)
            gather_send("gather1", x_all, "beside", j)

    for slot in range(complete_at(total - 1) + 1):
        advance(slot // 3, slot % 3 + 1)
        for function, args in work.get(slot, ()):
            function(*args)
    down_near(last)
    finish_down(last - 2)
    finish_down(last - 1)
    finish_down(last)
    for step in sorted(pending):
        finish_sends(step)
    for copy in y_pending:
        copy.wait_send()
    for c in range(down_chunks):
        out_copy(c).wait()


def layer(
    tokens, mix_gain, query_weight, key_weight, value_weight, gate_weight, out_weight, head_gain,
    ffn_gain, ffn_gate, ffn_up, ffn_down,
):
    bf16, f32 = jnp.bfloat16, jnp.float32
    rows, width = tokens.shape
    model = 4 * width
    seqs = rows // SEQ
    key_width, value_width = query_weight.shape[1], value_weight.shape[1]
    heads = head_gain.shape[0]
    mix_width = 2 * key_width + 2 * value_width
    hidden_width = ffn_gate.shape[1]
    blocks, down_chunks = hidden_width // LANES, ffn_down.shape[1] // LANES
    total = mix_width // (2 * LANES) + 1 + blocks + down_chunks + 1
    frequency = rope_base ** (-np.linspace(0.0, 1.0, DK // 2))
    angles = np.arange(SEQ)[:, None] * frequency[None, :]
    cosine = np.tile(np.repeat(np.cos(angles), 2, axis=1), (1, heads)).astype(np.float32)
    sine = np.tile(np.repeat(np.sin(angles), 2, axis=1), (1, heads)).astype(np.float32)
    rates = np.log1p(-np.exp2(-5.0 - 4.0 * np.arange(HEADS) / (HEADS - 1)))
    rates = np.broadcast_to(rates[:, None], (HEADS, SEQ)).astype(np.float32)
    anywhere = pl.BlockSpec(memory_space=pl.ANY)
    first_sum = [pltpu.VMEM((seqs, SEQ, width), bf16)] * 6
    second_sum = [pltpu.VMEM((down_chunks, rows, LANES), bf16)] * 6
    dma = pltpu.SemaphoreType.DMA
    return pl.pallas_call(
        fused_kernel,
        out_shape=jax.ShapeDtypeStruct((rows, width), bf16),
        in_specs=[anywhere] * 15,
        out_specs=anywhere,
        scratch_shapes=[
            pltpu.VMEM((1, model), f32),
            pltpu.VMEM(head_gain.shape, f32),
            pltpu.VMEM((1, model), f32),
            pltpu.VMEM(cosine.shape, f32),
            pltpu.VMEM(sine.shape, f32),
            pltpu.VMEM(rates.shape, f32),
            pltpu.VMEM((model, mix_width), bf16),
            pltpu.VMEM((out_weight.shape[0], model), bf16),
            pltpu.VMEM((model, 2 * hidden_width), bf16),
            pltpu.VMEM((down_chunks, hidden_width, 4 * LANES), bf16),
            pltpu.VMEM((rows, model), bf16),
            pltpu.VMEM((rows, model), bf16),
            pltpu.VMEM((SEQ, model), bf16),
            pltpu.VMEM((rows, model), bf16),
            pltpu.VMEM((SEQ, mix_width), bf16),
            pltpu.VMEM((SEQ, heads * DV), bf16),
            pltpu.VMEM((rows, hidden_width), bf16),
            pltpu.VMEM((heads, SEQ, SEQ), f32),
        ]
        + first_sum
        + [pltpu.VMEM((seqs, SEQ, width), f32)]
        + second_sum
        + [
            pltpu.VMEM((down_chunks, rows, LANES), f32),
            pltpu.VMEM((rows, LANES), f32),
            pltpu.VMEM((SEQ, 4 * LANES), f32),
            pltpu.VMEM((down_chunks, rows, LANES), bf16),
        ]
        + [
            dma((20 + down_chunks,)),
            dma((3, 2, 4)),
            dma((total, 3)),
            dma((3, 2, 3)),
            dma((total, 3)),
            dma((15 * seqs,)),
            dma((9 * seqs + 3 * seqs * down_chunks,)),
            dma((down_chunks,)),
        ],
        compiler_params=pltpu.CompilerParams(
            collective_id=0, has_side_effects=True, vmem_limit_bytes=67043328
        ),
        name="layer",
    )(
        tokens, mix_gain.reshape(1, -1), query_weight, key_weight, value_weight, gate_weight, out_weight,
        head_gain, ffn_gain.reshape(1, -1), ffn_gate, ffn_up, ffn_down, cosine, sine, rates,
    )


def solution(mesh):
    shape = mesh.shape
    small = shape["rep"] == 2 and shape["fs"] == 4 and shape["tp"] == 4
    return jax.shard_map(
        layer if small else per_device_plain,
        mesh=mesh,
        in_specs=(
            P(("rep", "fs"), "tp"),
            P(),
            P("fs", "tp"),
            P("fs", "tp"),
            P("fs", "tp"),
            P("fs", "tp"),
            P("tp", "fs"),
            P("tp", None),
            P(),
            P("fs", "tp"),
            P("fs", "tp"),
            P("tp", "fs"),
        ),
        out_specs=P(("rep", "fs"), "tp"),
        check_vma=False,
    )
```
